32 devices in a mesh: fs: 16 (over z, y, x), tp: 2 (over core).
Axes of the slice: x: 2, y: 2, z: 4, core: 2. Of those that a mesh axis runs over, the one named last changes fastest.
Arguments:
- tokens: bfloat16 [12288, 2048], P('fs'), may hold values from -6 to 6
- norm_gain: float32 [2048], replicated, may hold values from 0.1 to 1.9
- gate_weight: bfloat16 [2048, 5120], P('fs', 'tp'), may hold values from -0.125 to 0.125
- up_weight: bfloat16 [2048, 5120], P('fs', 'tp'), may hold values from -0.125 to 0.125
- down_weight: bfloat16 [5120, 2048], P('tp', 'fs'), may hold values from -0.078125 to 0.078125
Outputs:
- mixed: bfloat16 [12288, 2048], P(('fs', 'tp'))
The draws below stay inside these ranges and needn't reach their ends.
All inputs are finite; a program needn't handle non-finite values.
Results may differ from the reference program's by a relative error of at most 0.014.
Values may be sent and summed in bfloat16 or wider, within the bound.
A program may use at most 128 MiB of HBM per device.

```python
import jax
import jax.numpy as jnp
from jax import lax

D = 2048
FF = 5120
TOKENS = 12288
N_TP = 2


def levels(stream_key, dims, split, low, largest):
    level, own = 1.0, jax.random.fold_in(stream_key, 6)
    for dim, parts in split:
        steps = jnp.exp(jax.random.uniform(jax.random.fold_in(own, dim), (parts,), jnp.float32, low / len(split), largest / len(split)))
        level = level * jnp.repeat(steps, dims[dim] // parts).reshape([-1 if axis == dim else 1 for axis in range(len(dims))])
    return level


def noise(rng, shape, spread, bound, pieces=(), dtype=jnp.bfloat16):
    result = spread * jax.random.normal(rng, shape, jnp.float32)
    if pieces:
        result = result * levels(rng, shape, pieces, -0.22, 0.18)
    return jnp.clip(result, -bound, bound).astype(dtype)


def setup_inputs(seed: int = 0) -> dict:
    splits = jax.random.split(jax.random.key(seed), 6)
    tokens = noise(splits[0], (TOKENS, D), 1.0, 6.0, ((0, 16),))
    norm_gain = jnp.clip(1.0 + 0.18 * jax.random.normal(splits[1], (D,), jnp.float32), 0.1, 1.9)
    gate_weight = noise(splits[2], (D, FF), D ** -0.5, 0.125, ((0, 16), (1, 2)))
    up_weight = noise(splits[3], (D, FF), D ** -0.5, 0.125, ((0, 16), (1, 2)))
    down_weight = noise(splits[4], (FF, D), FF ** -0.5, 0.078125, ((0, 2), (1, 16)))
    return dict(tokens=tokens, norm_gain=norm_gain, gate_weight=gate_weight, up_weight=up_weight, down_weight=down_weight)


def reference(tokens, norm_gain, gate_weight, up_weight, down_weight):
    values = tokens.astype(jnp.float32)
    scale = lax.rsqrt(lax.optimization_barrier(jnp.mean(values * values, axis=-1, keepdims=True)) + 1e-06)
    normed = (values * scale * norm_gain).astype(jnp.bfloat16)
    gate_proj = jnp.dot(normed, gate_weight, preferred_element_type=jnp.float32)
    up_proj = jnp.dot(normed, up_weight, preferred_element_type=jnp.float32)
    hidden = (jax.nn.silu(gate_proj) * up_proj).astype(jnp.bfloat16)
    block = FF // N_TP
    total = jnp.zeros((tokens.shape[0], D), jnp.float32)
    for index in range(N_TP):
        part_sum = jnp.dot(hidden[:, index * block:(index + 1) * block], down_weight[index * block:(index + 1) * block, :], preferred_element_type=jnp.float32).astype(jnp.bfloat16)
        total = total + part_sum.astype(jnp.float32)
    return total.astype(jnp.bfloat16)
```

```python
import functools

import jax
import jax.numpy as jnp
from jax import lax
from jax.experimental import pallas as pl
from jax.experimental.pallas import tpu as pltpu
from jax.sharding import PartitionSpec as P

MESH = pl.DeviceIdType.MESH
PLANE = 4
ORDER = ((1, 1), (0, 1), (1, 0), (0, 0))


def simple(tokens, norm_gain, gate_weight, up_weight, down_weight):
    values = tokens.astype(jnp.float32)
    scale = lax.rsqrt(jnp.mean(values * values, axis=-1, keepdims=True) + 1e-06)
    normed = (values * scale * norm_gain).astype(jnp.bfloat16)

    def project(piece):
        whole = lax.all_gather(piece, "fs", axis=0, tiled=True)
        return jnp.dot(normed, whole, preferred_element_type=jnp.float32)

    hidden = (jax.nn.silu(project(gate_weight)) * project(up_weight)).astype(jnp.bfloat16)
    down_whole = lax.all_gather(down_weight, "fs", axis=1, tiled=True)
    return lax.psum_scatter(
        jnp.dot(hidden, down_whole, preferred_element_type=jnp.float32).astype(jnp.bfloat16),
        "tp",
        scatter_dimension=0,
        tiled=True,
    )


def kernel(nz, tok_hbm, gain_ref, gate_hbm, up_hbm, down_hbm, out_ref,
           tok, acc, gu, dn, hidden, psend, precv, own,
           loc_sem, a2a_s, a2a_r, tok_s, tok_r, up_s, dn_s, z_r, sib_s, sib_r, one_s, one_r, rs_s, rs_r):
    f = lax.axis_index("fs")
    c = lax.axis_index("tp")
    z, p = f // PLANE, f % PLANE
    y, x = p // 2, p % 2
    depth = gate_hbm.shape[0]
    width = gate_hbm.shape[1] // PLANE
    rows = tok_hbm.shape[0] // 2
    unit = depth * PLANE

    def member(k):
        oy, ox = ORDER[k]
        return ((y + oy) % 2) * 2 + (x + ox) % 2

    def dev(plane, z_, core):
        return (z_ * PLANE + plane, core)

    barrier = pltpu.get_barrier_semaphore()
    for k in range(3):
        pl.semaphore_signal(barrier, inc=1, device_id=dev(member(k), z, c), device_id_type=MESH)
    pl.semaphore_signal(barrier, inc=1, device_id=(f, 1 - c), device_id_type=MESH)

    @pl.when(z > 0)
    def _():
        pl.semaphore_signal(barrier, inc=1, device_id=dev(p, z - 1, c), device_id_type=MESH)

    @pl.when(z < nz - 1)
    def _():
        pl.semaphore_signal(barrier, inc=1, device_id=dev(p, z + 1, c), device_id_type=MESH)

    pl.semaphore_wait(barrier, 4 + (z + nz - 1) // nz + (2 * nz - 2 - z) // nz)

    sources = (gate_hbm, up_hbm, down_hbm)

    def piece_src(m, q):
        start = pl.multiple_of(q * width, 128)
        if m < 2:
            return sources[m].at[:, pl.ds(start, width)]
        return sources[m].at[pl.ds(start, width), :]

    def weight_dst(m, start, size):
        start = pl.multiple_of(start, 128)
        units = pl.ds(pl.multiple_of(c * width, 128), width)
        if m < 2:
            return gu.at[m, pl.ds(start, size), units]
        return dn.at[units, pl.ds(start, size)]

    def weight_sib(m, start, size):
        start = pl.multiple_of(start, 128)
        units = pl.ds(pl.multiple_of((1 - c) * width, 128), width)
        if m < 2:
            return gu.at[m, pl.ds(start, size), units]
        return dn.at[units, pl.ds(start, size)]

    def a2a(m, k):
        q = member(k)
        return pltpu.make_async_remote_copy(
            src_ref=piece_src(m, q), dst_ref=weight_dst(m, f * depth, depth),
            send_sem=a2a_s.at[m, k], recv_sem=a2a_r.at[m, k],
            device_id=dev(q, z, c), device_id_type=MESH)

    def a2a_in(m, k):
        q = member(k)
        ref = weight_dst(m, (z * PLANE + q) * depth, depth)
        return pltpu.make_async_remote_copy(
            src_ref=ref, dst_ref=ref, send_sem=a2a_s.at[m, k], recv_sem=a2a_r.at[m, k],
            device_id=dev(q, z, c), device_id_type=MESH)

    def local(m):
        return pltpu.make_async_copy(piece_src(m, p), weight_dst(m, f * depth, depth), loc_sem.at[m])

    half = pl.ds(pl.multiple_of(c * rows, 16), rows)
    part_rows = (pl.ds(0, rows // 2), pl.ds(rows // 2, rows // 2))

    def tok_part(k, h):
        ref = psend.at[k, part_rows[h], :]
        if k == 0:
            source, to = psend.at[1 + h, part_rows[h], :], member(2 - h)
        else:
            start = pl.multiple_of(c * rows + h * (rows // 2), 16)
            source, to = tok_hbm.at[pl.ds(start, rows // 2), :], member(k)
        return pltpu.make_async_remote_copy(
            src_ref=source, dst_ref=ref, send_sem=tok_s.at[k, h], recv_sem=tok_r.at[k, h],
            device_id=dev(to, z, c), device_id_type=MESH)

    own_tok = pltpu.make_async_copy(tok_hbm.at[half, :], tok.at[3], loc_sem.at[3])

    def along(m, zs, step):
        ref = weight_dst(m, zs * unit, unit)
        sems = up_s if step > 0 else dn_s
        return pltpu.make_async_remote_copy(
            src_ref=ref, dst_ref=ref, send_sem=sems.at[m, zs], recv_sem=z_r.at[m, zs],
            device_id=dev(p, z + step, c), device_id_type=MESH)

    def to_sibling(m, zs):
        ref = weight_dst(m, zs * unit, unit)
        return pltpu.make_async_remote_copy(
            src_ref=ref, dst_ref=ref, send_sem=sib_s.at[m, zs], recv_sem=sib_r.at[m, zs],
            device_id=(f, 1 - c), device_id_type=MESH)

    def from_sibling(m, zs):
        ref = weight_sib(m, zs * unit, unit)
        return pltpu.make_async_remote_copy(
            src_ref=ref, dst_ref=ref, send_sem=sib_s.at[m, zs], recv_sem=sib_r.at[m, zs],
            device_id=(f, 1 - c), device_id_type=MESH)

    def forward(m, zs):
        @pl.when((zs <= z) & (z < nz - 1))
        def _():
            along(m, zs, 1).start()

        @pl.when((zs >= z) & (z > 0))
        def _():
            along(m, zs, -1).start()

        to_sibling(m, zs).start()

    def arrived(m, zs):
        along(m, zs, 1).wait_recv()

    def piece(m, k, step):
        ref = weight_dst(m, (z * PLANE + member(k)) * depth, depth)
        sems = up_s if step > 0 else dn_s
        return pltpu.make_async_remote_copy(
            src_ref=piece_src(m, p) if k == 3 else ref, dst_ref=ref,
            send_sem=sems.at[m, z], recv_sem=z_r.at[m, z],
            device_id=dev(p, z + step, c), device_id_type=MESH)

    def pass_piece(m, k):
        @pl.when(z < nz - 1)
        def _():
            piece(m, k, 1).start()

        @pl.when(z > 0)
        def _():
            piece(m, k, -1).start()

    for m in range(2):
        for k in (1, 2, 0):
            a2a(m, k).start()
        local(m).start()
        pass_piece(m, 3)
    for h in range(2):
        tok_part(1, h).start()
        tok_part(2, 1 - h).start()
    own_tok.start()

    def own_unit(m):
        if m == 2:
            pass_piece(m, 3)
        for k in (1, 2, 0):
            a2a_in(m, k).wait_recv()
            pass_piece(m, k)
        local(m).wait()
        to_sibling(m, z).start()

    own_unit(0)
    own_unit(1)

    def relay(m, d):
        @pl.when(z - d >= 0)
        def _():
            arrived(m, z - d)
            forward(m, z - d)

        @pl.when(z + d < nz)
        def _():
            arrived(m, z + d)
            forward(m, z + d)

    side = z // (nz // 2)
    edge = z + side * (nz - 1 - 2 * z)
    late = (nz - 1) * (1 - side)
    inner = (z > 0) & (z < nz - 1)

    def normalize(k):
        raw = tok.at[k] if k == 3 else psend.at[k]
        block = rows // 6

        @pl.loop(0, 6)
        def _(i):
            at = pl.ds(pl.multiple_of(i * block, 16), block)
            values = raw[at, :].astype(jnp.float32)
            scale = lax.rsqrt(jnp.mean(values * values, axis=-1, keepdims=True) + 1e-06)
            tok[k, at, :] = (values * scale * gain_ref[...]).astype(jnp.bfloat16)

    tiles = 2 * width // 256

    def tile_at(i):
        j = c * (tiles - 1) + i * (1 - 2 * c)
        return pl.ds(pl.multiple_of(j * 256, 256), 256)

    def project(m, k, at, start, size):
        depths = pl.ds(pl.multiple_of(start * unit, 128), size * unit)
        return jnp.dot(tok[k, :, depths], gu[m, depths, at], preferred_element_type=jnp.float32)

    def early(k):
        @pl.loop(0, tiles)
        def _(i):
            at = tile_at(i)
            for m in range(2):
                acc[m, k, :, at] = project(m, k, at, side, nz - 1)

    relay(0, 1)
    relay(1, 1)
    for h in range(2):
        tok_part(1 + h, h).wait_recv()
        tok_part(0, h).start()
    for k in (1, 2, 0):
        a2a(2, k).start()
    local(2).start()
    own_tok.wait()
    normalize(3)
    relay(0, 2)
    for k in (1, 2):
        tok_part(k, 2 - k).wait_recv()
        normalize(k)
    relay(1, 2)
    for m in range(2):
        for i in range(nz - 1):
            from_sibling(m, side + i).wait_recv()
    for k in (3, 1, 2):
        early(k)
    for h in range(2):
        tok_part(0, h).wait_recv()
    normalize(0)
    early(0)
    own_unit(2)

    relay(0, nz - 1)
    from_sibling(0, late).wait_recv()
    for k in range(PLANE):
        @pl.loop(0, tiles)
        def _(i):
            at = tile_at(i)
            gate = acc[0, k, :, at] + project(0, k, at, late, 1)
            acc[0, k, :, at] = gate / (1.0 + jnp.exp(-gate))

    for h in range(2):
        tok_part(0, h).wait_send()
    relay(1, nz - 1)

    def make_hidden(k, start, stop):
        @pl.loop(start, stop)
        def _(i):
            at = tile_at(i)
            up = acc[1, k, :, at] + project(1, k, at, late, 1)
            hidden[k, :, at] = (acc[0, k, :, at] * up).astype(jnp.bfloat16)

    def first(h, step):
        at = (0, part_rows[h], columns_at(step))
        return pltpu.make_async_remote_copy(
            src_ref=psend.at[at], dst_ref=precv.at[at],
            send_sem=one_s.at[h, step], recv_sem=one_r.at[h, step],
            device_id=dev(member(1 + h), z, c), device_id_type=MESH)

    def last(k, h, step):
        at = (k, part_rows[h], columns_at(step))
        return pltpu.make_async_remote_copy(
            src_ref=psend.at[at], dst_ref=precv.at[at],
            send_sem=rs_s.at[2 * k + h - 2, step], recv_sem=rs_r.at[2 * k + h - 2, step],
            device_id=dev(member(k), z, c), device_id_type=MESH)

    def plane_at(step):
        near = (2 * edge - step + nz) // nz
        ahead = near * (1 - 2 * (step % 2)) * ((step + 1) // 2) + (1 - near) * (step - edge)
        return z + ahead * (1 - 2 * side)

    def columns_at(step):
        return pl.ds(pl.multiple_of(plane_at(step) * unit, 128), unit)

    def add_and_send(step):
        for h in range(2):
            k = 2 - h
            first(h, step).wait_recv()
            at = (part_rows[h], columns_at(step))
            psend[(k, *at)] = (
                psend[(k, *at)].astype(jnp.float32) + precv[(0, *at)].astype(jnp.float32)
            ).astype(jnp.bfloat16)
            last(k, h, step).start()

    for step in range(nz):
        zs = plane_at(step)
        if step > 0:
            @pl.when(jnp.logical_not(inner))
            def _():
                arrived(2, zs)
                to_sibling(2, zs).start()

        if step % 2 == 1:
            @pl.when(inner)
            def _():
                relay(2, (step + 1) // 2)

        if step == 0:
            for k in range(PLANE):
                make_hidden(k, 0, tiles // 2)
            from_sibling(1, late).wait_recv()
        from_sibling(2, zs).wait_recv()
        for k in range(PLANE):
            if step == 0:
                make_hidden(k, tiles // 2, tiles)

            @pl.loop(0, unit // 256)
            def _(j):
                at = pl.ds(pl.multiple_of(zs * unit + j * 256, 256), 256)
                part = jnp.dot(hidden[k], dn[:, at], preferred_element_type=jnp.float32)
                if k == 3:
                    own[:, at] = part
                else:
                    psend[k, :, at] = part.astype(jnp.bfloat16)

            if k == 0:
                first(0, step).start()
                first(1, step).start()
            elif k < 3:
                last(k, k - 1, step).start()
        if step == 0:
            add_and_send(0)
        elif step > 1:
            add_and_send(step - 1)
    add_and_send(nz - 1)

    for step in range(nz):
        for k in (1, 2):
            for h in range(2):
                last(k, h, step).wait_recv()

        @pl.loop(0, unit // 256)
        def _(j):
            at = pl.ds(pl.multiple_of(plane_at(step) * unit + j * 256, 256), 256)
            total = own[:, at]
            for k in (1, 2):
                total = total + precv[k, :, at].astype(jnp.float32)
            out_ref[:, at] = total.astype(out_ref.dtype)

    for m in range(3):
        for k in range(3):
            a2a(m, k).wait_send()
        for zs in range(nz):
            to_sibling(m, zs).wait_send()

            @pl.when((zs <= z) & (z < nz - 1))
            def _():
                along(m, zs, 1).wait_send()

            @pl.when((zs >= z) & (z > 0))
            def _():
                along(m, zs, -1).wait_send()
    for k in (1, 2):
        for h in range(2):
            tok_part(k, h).wait_send()
    for step in range(nz):
        for h in range(2):
            first(h, step).wait_send()
            for k in (1, 2):
                last(k, h, step).wait_send()


def fused(nfs, tokens, norm_gain, gate_weight, up_weight, down_weight):
    nz = nfs // PLANE
    features = tokens.shape[1]
    rows = tokens.shape[0] // 2
    width = gate_weight.shape[1] // PLANE
    any_spec = pl.BlockSpec(memory_space=pl.ANY)
    vmem_spec = pl.BlockSpec(memory_space=pltpu.VMEM)
    dma = pltpu.SemaphoreType.DMA
    bf16 = jnp.bfloat16
    return pl.pallas_call(
        functools.partial(kernel, nz),
        out_shape=jax.ShapeDtypeStruct((rows, features), bf16),
        in_specs=[any_spec, vmem_spec, any_spec, any_spec, any_spec],
        out_specs=vmem_spec,
        scratch_shapes=[
            pltpu.VMEM((PLANE, rows, features), bf16),
            pltpu.VMEM((2, PLANE, rows, 2 * width), jnp.float32),
            pltpu.VMEM((2, features, 2 * width), bf16),
            pltpu.VMEM((2 * width, features), bf16),
            pltpu.VMEM((PLANE, rows, 2 * width), bf16),
            pltpu.VMEM((3, rows, features), bf16),
            pltpu.VMEM((3, rows, features), bf16),
            pltpu.VMEM((rows, features), jnp.float32),
            dma((4,)), dma((3, 3)), dma((3, 3)), dma((3, 2)), dma((3, 2)),
            dma((3, nz)), dma((3, nz)), dma((3, nz)), dma((3, nz)), dma((3, nz)),
            dma((2, nz)), dma((2, nz)), dma((4, nz)), dma((4, nz)),
        ],
        compiler_params=pltpu.CompilerParams(
            collective_id=0, has_side_effects=True, vmem_limit_bytes=62 * 1024 * 1024
        ),
    )(tokens, norm_gain.reshape(1, features), gate_weight, up_weight, down_weight)


def per_device(nfs, ntp, tokens, norm_gain, gate_weight, up_weight, down_weight):
    rows, depth = tokens.shape[0] // 2, gate_weight.shape[0]
    fits = (
        ntp == 2
        and nfs % PLANE == 0
        and nfs == PLANE * PLANE
        and rows % 96 == 0
        and depth % 128 == 0
        and depth * nfs == tokens.shape[1]
        and gate_weight.shape[1] % (PLANE * 128) == 0
    )
    body = functools.partial(fused, nfs) if fits else simple
    return body(tokens, norm_gain, gate_weight, up_weight, down_weight)


def solution(mesh):
    in_specs = (P("fs", None), P(), P("fs", "tp"), P("fs", "tp"), P("tp", "fs"))
    out_specs = P(("fs", "tp"), None)
    body = functools.partial(per_device, mesh.shape["fs"], mesh.shape["tp"])
    return jax.shard_map(
        body, mesh=mesh, in_specs=in_specs, out_specs=out_specs, check_vma=False
    )
```

```python
import functools

import jax
import jax.numpy as jnp
from jax import lax
from jax.experimental import pallas as pl
from jax.experimental.pallas import tpu as pltpu
from jax.sharding import PartitionSpec as P

MESH = pl.DeviceIdType.MESH
PLANE = 4
ORDER = ((1, 1), (0, 1), (1, 0), (0, 0))


def simple(tokens, norm_gain, gate_weight, up_weight, down_weight):
    values = tokens.astype(jnp.float32)
    scale = lax.rsqrt(jnp.mean(values * values, axis=-1, keepdims=True) + 1e-06)
    normed = (values * scale * norm_gain).astype(jnp.bfloat16)

    def project(piece):
        whole = lax.all_gather(piece, "fs", axis=0, tiled=True)
        return jnp.dot(normed, whole, preferred_element_type=jnp.float32)

    hidden = (jax.nn.silu(project(gate_weight)) * project(up_weight)).astype(jnp.bfloat16)
    down_whole = lax.all_gather(down_weight, "fs", axis=1, tiled=True)
    return lax.psum_scatter(
        jnp.dot(hidden, down_whole, preferred_element_type=jnp.float32).astype(jnp.bfloat16),
        "tp",
        scatter_dimension=0,
        tiled=True,
    )


def kernel(nz, tok_hbm, gain_ref, gate_hbm, up_hbm, down_hbm, out_ref,
           tok, acc, gu, dn, hidden, psend, precv, own,
           loc_sem, a2a_s, a2a_r, tok_s, tok_r, up_s, dn_s, z_r, sib_s, sib_r, end_s, end_r, pair_s, pair_r,
           one_s, one_r, rs_s, rs_r):
    f = lax.axis_index("fs")
    c = lax.axis_index("tp")
    z, p = f // PLANE, f % PLANE
    y, x = p // 2, p % 2
    depth = gate_hbm.shape[0]
    width = gate_hbm.shape[1] // PLANE
    rows = tok_hbm.shape[0] // 2
    unit = depth * PLANE

    def member(k):
        oy, ox = ORDER[k]
        return ((y + oy) % 2) * 2 + (x + ox) % 2

    def dev(plane, z_, core):
        return (z_ * PLANE + plane, core)

    barrier = pltpu.get_barrier_semaphore()
    for k in range(3):
        pl.semaphore_signal(barrier, inc=1, device_id=dev(member(k), z, c), device_id_type=MESH)
    pl.semaphore_signal(barrier, inc=1, device_id=(f, 1 - c), device_id_type=MESH)

    @pl.when(z > 0)
    def _():
        pl.semaphore_signal(barrier, inc=1, device_id=dev(p, z - 1, c), device_id_type=MESH)

    @pl.when(z < nz - 1)
    def _():
        pl.semaphore_signal(barrier, inc=1, device_id=dev(p, z + 1, c), device_id_type=MESH)

    pl.semaphore_wait(barrier, 4 + (z + nz - 1) // nz + (2 * nz - 2 - z) // nz)

    sources = (gate_hbm, up_hbm, down_hbm)

    def piece_src(m, q):
        start = pl.multiple_of(q * width, 128)
        if m < 2:
            return sources[m].at[:, pl.ds(start, width)]
        return sources[m].at[pl.ds(start, width), :]

    def weight_dst(m, start, size):
        start = pl.multiple_of(start, 128)
        units = pl.ds(pl.multiple_of(c * width, 128), width)
        if m < 2:
            return gu.at[m, pl.ds(start, size), units]
        return dn.at[units, pl.ds(start, size)]

    def weight_sib(m, start, size):
        start = pl.multiple_of(start, 128)
        units = pl.ds(pl.multiple_of((1 - c) * width, 128), width)
        if m < 2:
            return gu.at[m, pl.ds(start, size), units]
        return dn.at[units, pl.ds(start, size)]

    def a2a(m, k):
        q = member(k)
        return pltpu.make_async_remote_copy(
            src_ref=piece_src(m, q), dst_ref=weight_dst(m, f * depth, depth),
            send_sem=a2a_s.at[m, k], recv_sem=a2a_r.at[m, k],
            device_id=dev(q, z, c), device_id_type=MESH)

    def a2a_in(m, k):
        q = member(k)
        ref = weight_dst(m, (z * PLANE + q) * depth, depth)
        return pltpu.make_async_remote_copy(
            src_ref=ref, dst_ref=ref, send_sem=a2a_s.at[m, k], recv_sem=a2a_r.at[m, k],
            device_id=dev(q, z, c), device_id_type=MESH)

    def local(m):
        return pltpu.make_async_copy(piece_src(m, p), weight_dst(m, f * depth, depth), loc_sem.at[m])

    half = pl.ds(pl.multiple_of(c * rows, 16), rows)
    part_rows = (pl.ds(0, rows // 2), pl.ds(rows // 2, rows // 2))

    def tok_part(k, h):
        ref = psend.at[k, part_rows[h], :]
        if k == 0:
            source, to = psend.at[1 + h, part_rows[h], :], member(2 - h)
        else:
            start = pl.multiple_of(c * rows + h * (rows // 2), 16)
            source, to = tok_hbm.at[pl.ds(start, rows // 2), :], member(k)
        return pltpu.make_async_remote_copy(
            src_ref=source, dst_ref=ref, send_sem=tok_s.at[k, h], recv_sem=tok_r.at[k, h],
            device_id=dev(to, z, c), device_id_type=MESH)

    own_tok = pltpu.make_async_copy(tok_hbm.at[half, :], tok.at[3], loc_sem.at[3])

    def along(m, zs, step):
        ref = weight_dst(m, zs * unit, unit)
        sems = up_s if step > 0 else dn_s
        return pltpu.make_async_remote_copy(
            src_ref=ref, dst_ref=ref, send_sem=sems.at[m, zs], recv_sem=z_r.at[m, zs],
            device_id=dev(p, z + step, c), device_id_type=MESH)

    def to_sibling(m, zs):
        ref = weight_dst(m, zs * unit, unit)
        return pltpu.make_async_remote_copy(
            src_ref=ref, dst_ref=ref, send_sem=sib_s.at[m, zs], recv_sem=sib_r.at[m, zs],
            device_id=(f, 1 - c), device_id_type=MESH)

    def from_sibling(m, zs):
        ref = weight_sib(m, zs * unit, unit)
        return pltpu.make_async_remote_copy(
            src_ref=ref, dst_ref=ref, send_sem=sib_s.at[m, zs], recv_sem=sib_r.at[m, zs],
            device_id=(f, 1 - c), device_id_type=MESH)

    def forward(m, zs):
        @pl.when((zs <= z) & (z < nz - 1))
        def _():
            along(m, zs, 1).start()

        @pl.when((zs >= z) & (z > 0))
        def _():
            along(m, zs, -1).start()

        to_sibling(m, zs).start()

    def arrived(m, zs):
        along(m, zs, 1).wait_recv()

    def piece(m, k, step):
        ref = weight_dst(m, (z * PLANE + member(k)) * depth, depth)
        sems = up_s if step > 0 else dn_s
        return pltpu.make_async_remote_copy(
            src_ref=piece_src(m, p) if k == 3 else ref, dst_ref=ref,
            send_sem=sems.at[m, z], recv_sem=z_r.at[m, z],
            device_id=dev(p, z + step, c), device_id_type=MESH)

    def pass_piece(m, k):
        @pl.when(z < nz - 1)
        def _():
            piece(m, k, 1).start()

        @pl.when(z > 0)
        def _():
            piece(m, k, -1).start()

    for m in range(2):
        for k in (1, 2, 0):
            a2a(m, k).start()
        local(m).start()
        pass_piece(m, 3)
    for h in range(2):
        tok_part(1, h).start()
        tok_part(2, 1 - h).start()
    own_tok.start()

    def own_unit(m):
        if m == 2:
            pass_piece(m, 3)
        for k in (1, 2, 0):
            a2a_in(m, k).wait_recv()
            pass_piece(m, k)
        local(m).wait()
        to_sibling(m, z).start()

    own_unit(0)
    own_unit(1)

    side = z // (nz // 2)
    edge = z + side * (nz - 1 - 2 * z)
    late = (nz - 1) * (1 - side)
    inner = (z > 0) & (z < nz - 1)
    outer = jnp.logical_not(inner)

    def end_half(m, h):
        ref = weight_dst(m, late * unit + h * (unit // 2), unit // 2)
        return pltpu.make_async_remote_copy(
            src_ref=ref, dst_ref=ref, send_sem=end_s.at[m - 1, h], recv_sem=end_r.at[m - 1, h],
            device_id=dev(p, z + 2 * side - 1, c), device_id_type=MESH)

    def pair_half(m, h, mine):
        where = weight_dst if mine else weight_sib
        ref = where(m, late * unit + h * (unit // 2), unit // 2)
        return pltpu.make_async_remote_copy(
            src_ref=ref, dst_ref=ref, send_sem=pair_s.at[m - 1, h], recv_sem=pair_r.at[m - 1, h],
            device_id=(f, 1 - c), device_id_type=MESH)

    def relay(m, d):
        @pl.when(z - d >= 0)
        def _():
            arrived(m, z - d)
            forward(m, z - d)

        @pl.when(z + d < nz)
        def _():
            arrived(m, z + d)
            forward(m, z + d)

    def relay_far(m):
        @pl.when(inner)
        def _():
            arrived(m, late)
            for h in range(2):
                end_half(m, h).start()
            to_sibling(m, late).start()

    def take(m, d):
        @pl.when(outer)
        def _():
            zs = z + d * (1 - 2 * side)
            arrived(m, zs)
            to_sibling(m, zs).start()

    def take_half(m, h):
        @pl.when(outer)
        def _():
            end_half(m, h).wait_recv()
            pair_half(m, h, True).start()

    def paired_half(m, h):
        @pl.when(outer)
        def _():
            pair_half(m, h, False).wait_recv()

        if h == 0:
            @pl.when(inner)
            def _():
                from_sibling(m, late).wait_recv()

    def normalize(k):
        raw = tok.at[k] if k == 3 else psend.at[k]
        block = rows // 6

        @pl.loop(0, 6)
        def _(i):
            at = pl.ds(pl.multiple_of(i * block, 16), block)
            values = raw[at, :].astype(jnp.float32)
            scale = lax.rsqrt(jnp.mean(values * values, axis=-1, keepdims=True) + 1e-06)
            tok[k, at, :] = (values * scale * gain_ref[...]).astype(jnp.bfloat16)

    tiles = 2 * width // 256

    def tile_at(i):
        j = c * (tiles - 1) + i * (1 - 2 * c)
        return pl.ds(pl.multiple_of(j * 256, 256), 256)

    def project(m, k, at, start, size):
        depths = pl.ds(pl.multiple_of(start, 128), size)
        return jnp.dot(tok[k, :, depths], gu[m, depths, at], preferred_element_type=jnp.float32)

    def early(m, k):
        @pl.loop(0, tiles)
        def _(i):
            at = tile_at(i)
            acc[m, k, :, at] = project(m, k, at, side * unit, (nz - 1) * unit)

    def all_paired(m):
        for i in range(nz - 1):
            from_sibling(m, side + i).wait_recv()

    relay(0, 1)
    relay(1, 1)
    for h in range(2):
        tok_part(1 + h, h).wait_recv()
        tok_part(0, h).start()
    for k in (1, 2, 0):
        a2a(2, k).start()
    local(2).start()
    own_tok.wait()
    normalize(3)
    relay(0, nz - 2)
    all_paired(0)
    early(0, 3)
    for k in (1, 2):
        tok_part(k, 2 - k).wait_recv()
        normalize(k)
        early(0, k)
    relay_far(1)
    take(1, nz - 2)
    all_paired(1)
    for k in (3, 1, 2):
        early(1, k)
    for h in range(2):
        tok_part(0, h).wait_recv()
    normalize(0)
    for m in range(2):
        early(m, 0)

    take(0, nz - 1)
    own_unit(2)
    from_sibling(0, late).wait_recv()
    for k in range(PLANE):
        @pl.loop(0, tiles)
        def _(i):
            at = tile_at(i)
            gate = acc[0, k, :, at] + project(0, k, at, late * unit, unit)
            acc[0, k, :, at] = gate / (1.0 + jnp.exp(-gate))

    take_half(1, 0)
    paired_half(1, 0)
    for k in range(PLANE):
        @pl.loop(0, tiles)
        def _(i):
            at = tile_at(i)
            acc[1, k, :, at] += project(1, k, at, late * unit, unit // 2)

    for h in range(2):
        tok_part(0, h).wait_send()
    take_half(1, 1)

    def make_hidden(k, start, stop):
        @pl.loop(start, stop)
        def _(i):
            at = tile_at(i)
            up = acc[1, k, :, at] + project(1, k, at, late * unit + unit // 2, unit // 2)
            hidden[k, :, at] = (acc[0, k, :, at] * up).astype(jnp.bfloat16)

    def first(h, step):
        at = (0, part_rows[h], columns_at(step))
        return pltpu.make_async_remote_copy(
            src_ref=psend.at[at], dst_ref=precv.at[at],
            send_sem=one_s.at[h, step], recv_sem=one_r.at[h, step],
            device_id=dev(member(1 + h), z, c), device_id_type=MESH)

    def last(k, h, step):
        at = (k, part_rows[h], columns_at(step))
        return pltpu.make_async_remote_copy(
            src_ref=psend.at[at], dst_ref=precv.at[at],
            send_sem=rs_s.at[2 * k + h - 2, step], recv_sem=rs_r.at[2 * k + h - 2, step],
            device_id=dev(member(k), z, c), device_id_type=MESH)

    def plane_at(step):
        near = (2 * edge - step + nz) // nz
        ahead = near * (1 - 2 * (step % 2)) * ((step + 1) // 2) + (1 - near) * (step - edge)
        return z + ahead * (1 - 2 * side)

    cuts = [(0, 0, 2), (0, 1, 2)] + [(step, 0, 1) for step in range(1, nz - 1)]
    cuts += [(nz - 1, 0, 2), (nz - 1, 1, 2)]

    def columns_at(i):
        step, part, parts = cuts[i]
        size = unit // parts
        return pl.ds(pl.multiple_of(plane_at(step) * unit + part * size, 128), size)

    def add_and_send(step):
        for h in range(2):
            k = 2 - h
            first(h, step).wait_recv()
            at = (part_rows[h], columns_at(step))
            psend[(k, *at)] = (
                psend[(k, *at)].astype(jnp.float32) + precv[(0, *at)].astype(jnp.float32)
            ).astype(jnp.bfloat16)
            last(k, h, step).start()

    def partials(i):
        step, part, parts = cuts[i]
        start, size = plane_at(step) * unit + part * (unit // parts), unit // parts
        for k in range(PLANE):
            if i == 0:
                make_hidden(k, tiles // 2, tiles)

            @pl.loop(0, size // 256)
            def _(j):
                at = pl.ds(pl.multiple_of(start + j * 256, 256), 256)
                part = jnp.dot(hidden[k], dn[:, at], preferred_element_type=jnp.float32)
                if k == 3:
                    own[:, at] = part
                else:
                    psend[k, :, at] = part.astype(jnp.bfloat16)

            if k == 0:
                first(0, i).start()
                first(1, i).start()
            elif k < 3:
                last(k, k - 1, i).start()

    for k in range(PLANE):
        make_hidden(k, 0, tiles // 2)
    paired_half(1, 1)
    from_sibling(2, z).wait_recv()
    final = len(cuts) - 1
    for i in range(final + 1):
        step, part, parts = cuts[i]
        if i == final:
            take_half(2, 1)
            paired_half(2, 1)
        elif i == final - 1:
            take_half(2, 0)
            paired_half(2, 0)
        elif step > 0:
            take(2, step)
            from_sibling(2, plane_at(step)).wait_recv()
        partials(i)
        if i == 0:
            continue
        if step == 0:
            @pl.when(inner)
            def _():
                relay(2, 1)
        elif step == nz - 2:
            relay_far(2)
        if i == 1:
            add_and_send(0)
        add_and_send(i)

    for i in range(final + 1):
        at = columns_at(i)
        for k in (1, 2):
            for h in range(2):
                last(k, h, i).wait_recv()
        total = own[:, at]
        for k in (1, 2):
            total = total + precv[k, :, at].astype(jnp.float32)
        out_ref[:, at] = total.astype(out_ref.dtype)

    for m in range(3):
        for k in range(3):
            a2a(m, k).wait_send()
        for zs in range(nz):
            whole = (zs - late) * (zs - late) > 0 if m > 0 else zs >= 0

            @pl.when(inner | whole)
            def _():
                to_sibling(m, zs).wait_send()

            @pl.when((zs <= z) & (z < nz - 1) & (outer | whole))
            def _():
                along(m, zs, 1).wait_send()

            @pl.when((zs >= z) & (z > 0) & (outer | whole))
            def _():
                along(m, zs, -1).wait_send()
    for m in (1, 2):
        for h in range(2):
            @pl.when(inner)
            def _():
                end_half(m, h).wait_send()

            @pl.when(outer)
            def _():
                pair_half(m, h, True).wait_send()
    for k in (1, 2):
        for h in range(2):
            tok_part(k, h).wait_send()
    for i in range(final + 1):
        for h in range(2):
            first(h, i).wait_send()
            for k in (1, 2):
                last(k, h, i).wait_send()


def fused(nfs, tokens, norm_gain, gate_weight, up_weight, down_weight):
    nz = nfs // PLANE
    features = tokens.shape[1]
    rows = tokens.shape[0] // 2
    width = gate_weight.shape[1] // PLANE
    any_spec = pl.BlockSpec(memory_space=pl.ANY)
    vmem_spec = pl.BlockSpec(memory_space=pltpu.VMEM)
    dma = pltpu.SemaphoreType.DMA
    bf16 = jnp.bfloat16
    return pl.pallas_call(
        functools.partial(kernel, nz),
        out_shape=pltpu.VMEM((rows, features), bf16),
        in_specs=[any_spec, vmem_spec, any_spec, any_spec, any_spec],
        out_specs=vmem_spec,
        scratch_shapes=[
            pltpu.VMEM((PLANE, rows, features), bf16),
            pltpu.VMEM((2, PLANE, rows, 2 * width), jnp.float32),
            pltpu.VMEM((2, features, 2 * width), bf16),
            pltpu.VMEM((2 * width, features), bf16),
            pltpu.VMEM((PLANE, rows, 2 * width), bf16),
            pltpu.VMEM((3, rows, features), bf16),
            pltpu.VMEM((3, rows, features), bf16),
            pltpu.VMEM((rows, features), jnp.float32),
            dma((4,)), dma((3, 3)), dma((3, 3)), dma((3, 2)), dma((3, 2)),
            dma((3, nz)), dma((3, nz)), dma((3, nz)), dma((3, nz)), dma((3, nz)),
            dma((2, 2)), dma((2, 2)), dma((2, 2)), dma((2, 2)),
            dma((2, nz + 2)), dma((2, nz + 2)), dma((4, nz + 2)), dma((4, nz + 2)),
        ],
        compiler_params=pltpu.CompilerParams(
            collective_id=0, has_side_effects=True, vmem_limit_bytes=60 * 1024 * 1024
        ),
    )(tokens, norm_gain.reshape(1, features), gate_weight, up_weight, down_weight)


def per_device(nfs, ntp, tokens, norm_gain, gate_weight, up_weight, down_weight):
    rows, depth = tokens.shape[0] // 2, gate_weight.shape[0]
    fits = (
        ntp == 2
        and nfs % PLANE == 0
        and nfs == PLANE * PLANE
        and rows % 96 == 0
        and depth % 128 == 0
        and depth * nfs == tokens.shape[1]
        and gate_weight.shape[1] % (PLANE * 128) == 0
    )
    body = functools.partial(fused, nfs) if fits else simple
    return body(tokens, norm_gain, gate_weight, up_weight, down_weight)


def solution(mesh):
    in_specs = (P("fs", None), P(), P("fs", "tp"), P("fs", "tp"), P("tp", "fs"))
    out_specs = P(("fs", "tp"), None)
    body = functools.partial(per_device, mesh.shape["fs"], mesh.shape["tp"])
    return jax.shard_map(
        body, mesh=mesh, in_specs=in_specs, out_specs=out_specs, check_vma=False
    )
```

```python
import functools

import jax
import jax.numpy as jnp
from jax import lax
from jax.experimental import pallas as pl
from jax.experimental.pallas import tpu as pltpu
from jax.sharding import PartitionSpec as P

MESH = pl.DeviceIdType.MESH
PLANE = 4
ORDER = ((1, 1), (0, 1), (1, 0), (0, 0))


def simple(tokens, norm_gain, gate_weight, up_weight, down_weight):
    values = tokens.astype(jnp.float32)
    scale = lax.rsqrt(jnp.mean(values * values, axis=-1, keepdims=True) + 1e-06)
    normed = (values * scale * norm_gain).astype(jnp.bfloat16)

    def project(piece):
        whole = lax.all_gather(piece, "fs", axis=0, tiled=True)
        return jnp.dot(normed, whole, preferred_element_type=jnp.float32)

    hidden = (jax.nn.silu(project(gate_weight)) * project(up_weight)).astype(jnp.bfloat16)
    down_whole = lax.all_gather(down_weight, "fs", axis=1, tiled=True)
    return lax.psum_scatter(
        jnp.dot(hidden, down_whole, preferred_element_type=jnp.float32).astype(jnp.bfloat16),
        "tp",
        scatter_dimension=0,
        tiled=True,
    )


def kernel(nz, tok_hbm, gain_ref, gate_hbm, up_hbm, down_hbm, out_ref,
           tok, acc, gu, dn, hidden, psend, precv, own,
           loc_sem, a2a_s, a2a_r, tok_s, tok_r, up_s, dn_s, z_r, sib_s, sib_r, end_s, end_r, pair_s, pair_r, mid_s,
           one_s, one_r, rs_s, rs_r):
    f = lax.axis_index("fs")
    c = lax.axis_index("tp")
    z, p = f // PLANE, f % PLANE
    y, x = p // 2, p % 2
    depth = gate_hbm.shape[0]
    width = gate_hbm.shape[1] // PLANE
    rows = tok_hbm.shape[0] // 2
    unit = depth * PLANE

    def member(k):
        oy, ox = ORDER[k]
        return ((y + oy) % 2) * 2 + (x + ox) % 2

    def dev(plane, z_, core):
        return (z_ * PLANE + plane, core)

    barrier = pltpu.get_barrier_semaphore()
    for k in range(3):
        pl.semaphore_signal(barrier, inc=1, device_id=dev(member(k), z, c), device_id_type=MESH)
    pl.semaphore_signal(barrier, inc=1, device_id=(f, 1 - c), device_id_type=MESH)

    @pl.when(z > 0)
    def _():
        pl.semaphore_signal(barrier, inc=1, device_id=dev(p, z - 1, c), device_id_type=MESH)

    @pl.when(z < nz - 1)
    def _():
        pl.semaphore_signal(barrier, inc=1, device_id=dev(p, z + 1, c), device_id_type=MESH)

    pl.semaphore_wait(barrier, 4 + (z + nz - 1) // nz + (2 * nz - 2 - z) // nz)

    sources = (gate_hbm, up_hbm, down_hbm)

    def piece_src(m, q):
        start = pl.multiple_of(q * width, 128)
        if m < 2:
            return sources[m].at[:, pl.ds(start, width)]
        return sources[m].at[pl.ds(start, width), :]

    def weight_dst(m, start, size):
        start = pl.multiple_of(start, 128)
        units = pl.ds(pl.multiple_of(c * width, 128), width)
        if m < 2:
            return gu.at[m, pl.ds(start, size), units]
        return dn.at[units, pl.ds(start, size)]

    def weight_sib(m, start, size):
        start = pl.multiple_of(start, 128)
        units = pl.ds(pl.multiple_of((1 - c) * width, 128), width)
        if m < 2:
            return gu.at[m, pl.ds(start, size), units]
        return dn.at[units, pl.ds(start, size)]

    def a2a(m, k):
        q = member(k)
        return pltpu.make_async_remote_copy(
            src_ref=piece_src(m, q), dst_ref=weight_dst(m, f * depth, depth),
            send_sem=a2a_s.at[m, k], recv_sem=a2a_r.at[m, k],
            device_id=dev(q, z, c), device_id_type=MESH)

    def a2a_in(m, k):
        q = member(k)
        ref = weight_dst(m, (z * PLANE + q) * depth, depth)
        return pltpu.make_async_remote_copy(
            src_ref=ref, dst_ref=ref, send_sem=a2a_s.at[m, k], recv_sem=a2a_r.at[m, k],
            device_id=dev(q, z, c), device_id_type=MESH)

    def local(m):
        return pltpu.make_async_copy(piece_src(m, p), weight_dst(m, f * depth, depth), loc_sem.at[m])

    half = pl.ds(pl.multiple_of(c * rows, 16), rows)
    part_rows = (pl.ds(0, rows // 2), pl.ds(rows // 2, rows // 2))

    def tok_part(k, h):
        ref = psend.at[k, part_rows[h], :]
        if k == 0:
            source, to = psend.at[1 + h, part_rows[h], :], member(2 - h)
        else:
            start = pl.multiple_of(c * rows + h * (rows // 2), 16)
            source, to = tok_hbm.at[pl.ds(start, rows // 2), :], member(k)
        return pltpu.make_async_remote_copy(
            src_ref=source, dst_ref=ref, send_sem=tok_s.at[k, h], recv_sem=tok_r.at[k, h],
            device_id=dev(to, z, c), device_id_type=MESH)

    own_tok = pltpu.make_async_copy(tok_hbm.at[half, :], tok.at[3], loc_sem.at[3])

    def along(m, zs, step):
        ref = weight_dst(m, zs * unit, unit)
        sems = up_s if step > 0 else dn_s
        return pltpu.make_async_remote_copy(
            src_ref=ref, dst_ref=ref, send_sem=sems.at[m, zs], recv_sem=z_r.at[m, zs],
            device_id=dev(p, z + step, c), device_id_type=MESH)

    def to_sibling(m, zs):
        ref = weight_dst(m, zs * unit, unit)
        return pltpu.make_async_remote_copy(
            src_ref=ref, dst_ref=ref, send_sem=sib_s.at[m, zs], recv_sem=sib_r.at[m, zs],
            device_id=(f, 1 - c), device_id_type=MESH)

    def from_sibling(m, zs):
        ref = weight_sib(m, zs * unit, unit)
        return pltpu.make_async_remote_copy(
            src_ref=ref, dst_ref=ref, send_sem=sib_s.at[m, zs], recv_sem=sib_r.at[m, zs],
            device_id=(f, 1 - c), device_id_type=MESH)

    def forward(m, zs):
        @pl.when((zs <= z) & (z < nz - 1))
        def _():
            along(m, zs, 1).start()

        @pl.when((zs >= z) & (z > 0))
        def _():
            along(m, zs, -1).start()

        to_sibling(m, zs).start()

    def arrived(m, zs):
        along(m, zs, 1).wait_recv()

    def piece(m, k, step):
        ref = weight_dst(m, (z * PLANE + member(k)) * depth, depth)
        sems = up_s if step > 0 else dn_s
        return pltpu.make_async_remote_copy(
            src_ref=piece_src(m, p) if k == 3 else ref, dst_ref=ref,
            send_sem=sems.at[m, z], recv_sem=z_r.at[m, z],
            device_id=dev(p, z + step, c), device_id_type=MESH)

    def pass_piece(m, k):
        @pl.when(z < nz - 1)
        def _():
            piece(m, k, 1).start()

        @pl.when(z > 0)
        def _():
            piece(m, k, -1).start()

    for m in range(2):
        for k in (1, 2, 0):
            a2a(m, k).start()
        local(m).start()
        pass_piece(m, 3)
    for h in range(2):
        tok_part(1, h).start()
        tok_part(2, 1 - h).start()
    own_tok.start()

    def own_unit(m):
        if m == 2:
            pass_piece(m, 3)
        for k in (1, 2, 0):
            a2a_in(m, k).wait_recv()
            pass_piece(m, k)
        local(m).wait()
        to_sibling(m, z).start()

    own_unit(0)
    own_unit(1)

    side = z // (nz // 2)
    edge = z + side * (nz - 1 - 2 * z)
    late = (nz - 1) * (1 - side)
    inner = (z > 0) & (z < nz - 1)
    outer = jnp.logical_not(inner)

    def end_half(m, zs, h):
        ref = weight_dst(m, zs * unit + h * (unit // 2), unit // 2)
        return pltpu.make_async_remote_copy(
            src_ref=ref, dst_ref=ref, send_sem=end_s.at[m - 1, zs, h], recv_sem=end_r.at[m - 1, zs, h],
            device_id=dev(p, z + 2 * side - 1, c), device_id_type=MESH)

    def pair_half(m, zs, h, mine):
        where = weight_dst if mine else weight_sib
        ref = where(m, zs * unit + h * (unit // 2), unit // 2)
        return pltpu.make_async_remote_copy(
            src_ref=ref, dst_ref=ref, send_sem=pair_s.at[m - 1, zs, h], recv_sem=pair_r.at[m - 1, zs, h],
            device_id=(f, 1 - c), device_id_type=MESH)

    def across(zs, start, size):
        ref = weight_dst(2, start, size)
        return pltpu.make_async_remote_copy(
            src_ref=ref, dst_ref=ref, send_sem=mid_s.at[zs], recv_sem=z_r.at[2, zs],
            device_id=dev(p, z + 1 - 2 * side, c), device_id_type=MESH)

    def piece_out(q):
        start = (z * PLANE + q) * depth
        across(z, start, depth).start()
        ref = weight_dst(2, start, depth)
        half_at = 2 * q // PLANE
        pltpu.make_async_remote_copy(
            src_ref=ref, dst_ref=ref, send_sem=end_s.at[1, z, half_at], recv_sem=end_r.at[1, z, half_at],
            device_id=dev(p, z + 2 * side - 1, c), device_id_type=MESH).start()

    def own_down():
        for k in (1, 2, 0):
            a2a_in(2, k).wait_recv()
        local(2).wait()
        to_sibling(2, z).start()

        @pl.when(outer)
        def _():
            for k in range(PLANE):
                pass_piece(2, k)

        @pl.when(inner)
        def _():
            for q in range(PLANE):
                piece_out(q)

    def relay(m, d):
        @pl.when(z - d >= 0)
        def _():
            arrived(m, z - d)
            forward(m, z - d)

        @pl.when(z + d < nz)
        def _():
            arrived(m, z + d)
            forward(m, z + d)

    def relay_far(m):
        @pl.when(inner)
        def _():
            arrived(m, late)
            for h in range(2):
                end_half(m, late, h).start()
            to_sibling(m, late).start()

    def relay_near():
        @pl.when(inner)
        def _():
            zs = z + 1 - 2 * side
            arrived(2, zs)
            for h in range(2):
                end_half(2, zs, h).start()
            to_sibling(2, zs).start()
            zs = z + 2 * side - 1
            arrived(2, zs)
            across(zs, zs * unit, unit).start()
            to_sibling(2, zs).start()

    def take(m, d):
        @pl.when(outer)
        def _():
            zs = z + d * (1 - 2 * side)
            arrived(m, zs)
            to_sibling(m, zs).start()

    def take_half(m, zs, h):
        @pl.when(outer)
        def _():
            end_half(m, zs, h).wait_recv()
            pair_half(m, zs, h, True).start()

    def paired_half(m, zs, h):
        @pl.when(outer)
        def _():
            pair_half(m, zs, h, False).wait_recv()

        if h == 0:
            @pl.when(inner)
            def _():
                from_sibling(m, zs).wait_recv()

    def normalize(k):
        raw = tok.at[k] if k == 3 else psend.at[k]
        block = rows // 6

        @pl.loop(0, 6)
        def _(i):
            at = pl.ds(pl.multiple_of(i * block, 16), block)
            values = raw[at, :].astype(jnp.float32)
            scale = lax.rsqrt(jnp.mean(values * values, axis=-1, keepdims=True) + 1e-06)
            tok[k, at, :] = (values * scale * gain_ref[...]).astype(jnp.bfloat16)

    tiles = 2 * width // 256

    def tile_at(i):
        j = c * (tiles - 1) + i * (1 - 2 * c)
        return pl.ds(pl.multiple_of(j * 256, 256), 256)

    def project(m, k, at, start, size):
        depths = pl.ds(pl.multiple_of(start, 128), size)
        return jnp.dot(tok[k, :, depths], gu[m, depths, at], preferred_element_type=jnp.float32)

    def early(m, k):
        @pl.loop(0, tiles)
        def _(i):
            at = tile_at(i)
            acc[m, k, :, at] = project(m, k, at, side * unit, (nz - 1) * unit)

    def all_paired(m):
        for i in range(nz - 1):
            from_sibling(m, side + i).wait_recv()

    relay(0, 1)
    relay(1, 1)
    for h in range(2):
        tok_part(1 + h, h).wait_recv()
        tok_part(0, h).start()
    for k in (1, 2, 0):
        a2a(2, k).start()
    local(2).start()
    own_tok.wait()
    normalize(3)
    relay(0, nz - 2)
    all_paired(0)
    early(0, 3)
    for k in (1, 2):
        tok_part(k, 2 - k).wait_recv()
        normalize(k)
        early(0, k)
    relay_far(1)
    take(1, nz - 2)
    all_paired(1)
    for k in (3, 1, 2):
        early(1, k)
    for h in range(2):
        tok_part(0, h).wait_recv()
    normalize(0)
    for m in range(2):
        early(m, 0)

    take(0, nz - 1)
    own_down()
    from_sibling(0, late).wait_recv()
    for k in range(PLANE):
        @pl.loop(0, tiles)
        def _(i):
            at = tile_at(i)
            gate = acc[0, k, :, at] + project(0, k, at, late * unit, unit)
            acc[0, k, :, at] = gate / (1.0 + jnp.exp(-gate))

    take_half(1, late, 0)
    paired_half(1, late, 0)
    for k in range(PLANE):
        @pl.loop(0, tiles)
        def _(i):
            at = tile_at(i)
            acc[1, k, :, at] += project(1, k, at, late * unit, unit // 2)

    for h in range(2):
        tok_part(0, h).wait_send()
    take_half(1, late, 1)

    def make_hidden(k, start, stop):
        @pl.loop(start, stop)
        def _(i):
            at = tile_at(i)
            up = acc[1, k, :, at] + project(1, k, at, late * unit + unit // 2, unit // 2)
            hidden[k, :, at] = (acc[0, k, :, at] * up).astype(jnp.bfloat16)

    def first(h, step):
        at = (0, part_rows[h], columns_at(step))
        return pltpu.make_async_remote_copy(
            src_ref=psend.at[at], dst_ref=precv.at[at],
            send_sem=one_s.at[h, step], recv_sem=one_r.at[h, step],
            device_id=dev(member(1 + h), z, c), device_id_type=MESH)

    def last(k, h, step):
        at = (k, part_rows[h], columns_at(step))
        return pltpu.make_async_remote_copy(
            src_ref=psend.at[at], dst_ref=precv.at[at],
            send_sem=rs_s.at[2 * k + h - 2, step], recv_sem=rs_r.at[2 * k + h - 2, step],
            device_id=dev(member(k), z, c), device_id_type=MESH)

    def plane_at(step):
        near = (2 * edge - step + nz) // nz
        ahead = near * (1 - 2 * (step % 2)) * ((step + 1) // 2) + (1 - near) * (step - edge)
        return z + ahead * (1 - 2 * side)

    def columns_at(i):
        size = unit // 2
        return pl.ds(pl.multiple_of(plane_at(i // 2) * unit + i % 2 * size, 128), size)

    def add_and_send(step):
        for h in range(2):
            k = 2 - h
            first(h, step).wait_recv()
            at = (part_rows[h], columns_at(step))
            psend[(k, *at)] = (
                psend[(k, *at)].astype(jnp.float32) + precv[(0, *at)].astype(jnp.float32)
            ).astype(jnp.bfloat16)
            last(k, h, step).start()

    def partials(i):
        start = plane_at(i // 2) * unit + i % 2 * (unit // 2)

        def down(low, high):
            @pl.loop(0, unit // 512)
            def _(j):
                at = pl.ds(pl.multiple_of(start + j * 256, 256), 256)
                left = hidden[low:high].reshape((high - low) * rows, 2 * width)
                part = jnp.dot(left, dn[:, at], preferred_element_type=jnp.float32)
                for k in range(low, high):
                    block = part[(k - low) * rows:(k - low + 1) * rows]
                    if k == 3:
                        own[:, at] = block
                    else:
                        psend[k, :, at] = block.astype(jnp.bfloat16)

        if i == 0:
            make_hidden(0, tiles // 2, tiles)
        down(0, 1)
        first(0, i).start()
        first(1, i).start()
        if i == 0:
            make_hidden(1, tiles // 2, tiles)
            make_hidden(2, tiles // 2, tiles)
            down(1, 3)
        else:
            down(1, 4)
        last(1, 0, i).start()
        last(2, 1, i).start()
        if i == 0:
            make_hidden(3, 0, tiles)
            down(3, 4)

    for k in range(3):
        make_hidden(k, 0, tiles // 2)
    paired_half(1, late, 1)
    from_sibling(2, z).wait_recv()
    final = 2 * nz - 1
    for i in range(final + 1):
        if i > 1:
            paired_half(2, plane_at(i // 2), i % 2)
        partials(i)
        if i == 1:
            relay_near()
        if i == 4:
            relay_far(2)
        if i > 0:
            add_and_send(i - 1)
        if 0 < i < final:
            take_half(2, plane_at((i + 1) // 2), (i + 1) % 2)
    add_and_send(final)

    for i in range(final + 1):
        at = columns_at(i)
        for k in (1, 2):
            for h in range(2):
                last(k, h, i).wait_recv()
        total = own[:, at]
        for k in (1, 2):
            total = total + precv[k, :, at].astype(jnp.float32)
        out_ref[:, at] = total.astype(out_ref.dtype)

    for m in range(3):
        for k in range(3):
            a2a(m, k).wait_send()
        for zs in range(nz):
            whole = (zs >= 0, (zs - late) * (zs - late) > 0, zs == z)[m]

            @pl.when(inner | whole)
            def _():
                to_sibling(m, zs).wait_send()

            @pl.when((zs <= z) & (z < nz - 1) & (outer | whole if m < 2 else outer))
            def _():
                along(m, zs, 1).wait_send()

            @pl.when((zs >= z) & (z > 0) & (outer | whole if m < 2 else outer))
            def _():
                along(m, zs, -1).wait_send()
    for h in range(2):
        @pl.when(inner)
        def _():
            end_half(1, late, h).wait_send()
            for zs in (z, z + 1 - 2 * side, late):
                end_half(2, zs, h).wait_send()

        @pl.when(outer)
        def _():
            pair_half(1, late, h, True).wait_send()
            for d in range(1, nz):
                pair_half(2, z + d * (1 - 2 * side), h, True).wait_send()

    @pl.when(inner)
    def _():
        for zs in (z, z + 2 * side - 1):
            across(zs, zs * unit, unit).wait_send()
    for k in (1, 2):
        for h in range(2):
            tok_part(k, h).wait_send()
    for i in range(final + 1):
        for h in range(2):
            first(h, i).wait_send()
            for k in (1, 2):
                last(k, h, i).wait_send()


def fused(nfs, tokens, norm_gain, gate_weight, up_weight, down_weight):
    nz = nfs // PLANE
    features = tokens.shape[1]
    rows = tokens.shape[0] // 2
    width = gate_weight.shape[1] // PLANE
    any_spec = pl.BlockSpec(memory_space=pl.ANY)
    vmem_spec = pl.BlockSpec(memory_space=pltpu.VMEM)
    dma = pltpu.SemaphoreType.DMA
    bf16 = jnp.bfloat16
    return pl.pallas_call(
        functools.partial(kernel, nz),
        out_shape=pltpu.VMEM((rows, features), bf16),
        in_specs=[any_spec, vmem_spec, any_spec, any_spec, any_spec],
        out_specs=vmem_spec,
        scratch_shapes=[
            pltpu.VMEM((PLANE, rows, features), bf16),
            pltpu.VMEM((2, PLANE, rows, 2 * width), jnp.float32),
            pltpu.VMEM((2, features, 2 * width), bf16),
            pltpu.VMEM((2 * width, features), bf16),
            pltpu.VMEM((PLANE, rows, 2 * width), bf16),
            pltpu.VMEM((3, rows, features), bf16),
            pltpu.VMEM((3, rows, features), bf16),
            pltpu.VMEM((rows, features), jnp.float32),
            dma((4,)), dma((3, 3)), dma((3, 3)), dma((3, 2)), dma((3, 2)),
            dma((3, nz)), dma((3, nz)), dma((3, nz)), dma((3, nz)), dma((3, nz)),
            dma((2, nz, 2)), dma((2, nz, 2)), dma((2, nz, 2)), dma((2, nz, 2)), dma((nz,)),
            dma((2, 2 * nz)), dma((2, 2 * nz)), dma((4, 2 * nz)), dma((4, 2 * nz)),
        ],
        compiler_params=pltpu.CompilerParams(
            collective_id=0, has_side_effects=True, vmem_limit_bytes=60 * 1024 * 1024
        ),
    )(tokens, norm_gain.reshape(1, features), gate_weight, up_weight, down_weight)


def per_device(nfs, ntp, tokens, norm_gain, gate_weight, up_weight, down_weight):
    rows, depth = tokens.shape[0] // 2, gate_weight.shape[0]
    fits = (
        ntp == 2
        and nfs % PLANE == 0
        and nfs == PLANE * PLANE
        and rows % 96 == 0
        and depth % 128 == 0
        and depth * nfs == tokens.shape[1]
        and gate_weight.shape[1] % (PLANE * 128) == 0
    )
    body = functools.partial(fused, nfs) if fits else simple
    return body(tokens, norm_gain, gate_weight, up_weight, down_weight)


def solution(mesh):
    in_specs = (P("fs", None), P(), P("fs", "tp"), P("fs", "tp"), P("tp", "fs"))
    out_specs = P(("fs", "tp"), None)
    body = functools.partial(per_device, mesh.shape["fs"], mesh.shape["tp"])
    return jax.shard_map(
        body, mesh=mesh, in_specs=in_specs, out_specs=out_specs, check_vma=False
    )
```

```python
import functools

import jax
import jax.numpy as jnp
from jax import lax
from jax.experimental import pallas as pl
from jax.experimental.pallas import tpu as pltpu
from jax.sharding import PartitionSpec as P

MESH = pl.DeviceIdType.MESH
PLANE = 4
ORDER = ((1, 1), (0, 1), (1, 0), (0, 0))


def simple(tokens, norm_gain, gate_weight, up_weight, down_weight):
    values = tokens.astype(jnp.float32)
    scale = lax.rsqrt(jnp.mean(values * values, axis=-1, keepdims=True) + 1e-06)
    normed = (values * scale * norm_gain).astype(jnp.bfloat16)

    def project(piece):
        whole = lax.all_gather(piece, "fs", axis=0, tiled=True)
        return jnp.dot(normed, whole, preferred_element_type=jnp.float32)

    hidden = (jax.nn.silu(project(gate_weight)) * project(up_weight)).astype(jnp.bfloat16)
    down_whole = lax.all_gather(down_weight, "fs", axis=1, tiled=True)
    return lax.psum_scatter(
        jnp.dot(hidden, down_whole, preferred_element_type=jnp.float32).astype(jnp.bfloat16),
        "tp",
        scatter_dimension=0,
        tiled=True,
    )


def kernel(nz, tok_hbm, gain_ref, gate_hbm, up_hbm, down_hbm, out_ref,
           tok, acc, gu, dn, hidden, psend, precv, own, detour,
           loc_sem, a2a_s, a2a_r, tok_s, tok_r, up_s, dn_s, z_r, sib_s, sib_r, end_s, end_r, pair_s, pair_r, mid_s,
           one_s, one_r, rs_s, rs_r, det_s, det_r):
    f = lax.axis_index("fs")
    c = lax.axis_index("tp")
    z, p = f // PLANE, f % PLANE
    y, x = p // 2, p % 2
    depth = gate_hbm.shape[0]
    width = gate_hbm.shape[1] // PLANE
    rows = tok_hbm.shape[0] // 2
    unit = depth * PLANE

    def member(k):
        oy, ox = ORDER[k]
        return ((y + oy) % 2) * 2 + (x + ox) % 2

    def dev(plane, z_, core):
        return (z_ * PLANE + plane, core)

    barrier = pltpu.get_barrier_semaphore()
    for k in range(3):
        pl.semaphore_signal(barrier, inc=1, device_id=dev(member(k), z, c), device_id_type=MESH)
    pl.semaphore_signal(barrier, inc=1, device_id=(f, 1 - c), device_id_type=MESH)

    @pl.when(z > 0)
    def _():
        pl.semaphore_signal(barrier, inc=1, device_id=dev(p, z - 1, c), device_id_type=MESH)

    @pl.when(z < nz - 1)
    def _():
        pl.semaphore_signal(barrier, inc=1, device_id=dev(p, z + 1, c), device_id_type=MESH)

    pl.semaphore_wait(barrier, 4 + (z + nz - 1) // nz + (2 * nz - 2 - z) // nz)

    sources = (gate_hbm, up_hbm, down_hbm)

    def piece_src(m, q):
        start = pl.multiple_of(q * width, 128)
        if m < 2:
            return sources[m].at[:, pl.ds(start, width)]
        return sources[m].at[pl.ds(start, width), :]

    def weight_dst(m, start, size):
        start = pl.multiple_of(start, 128)
        units = pl.ds(pl.multiple_of(c * width, 128), width)
        if m < 2:
            return gu.at[m, pl.ds(start, size), units]
        return dn.at[units, pl.ds(start, size)]

    def weight_sib(m, start, size):
        start = pl.multiple_of(start, 128)
        units = pl.ds(pl.multiple_of((1 - c) * width, 128), width)
        if m < 2:
            return gu.at[m, pl.ds(start, size), units]
        return dn.at[units, pl.ds(start, size)]

    def a2a(m, k):
        q = member(k)
        return pltpu.make_async_remote_copy(
            src_ref=piece_src(m, q), dst_ref=weight_dst(m, f * depth, depth),
            send_sem=a2a_s.at[m, k], recv_sem=a2a_r.at[m, k],
            device_id=dev(q, z, c), device_id_type=MESH)

    def a2a_in(m, k):
        q = member(k)
        ref = weight_dst(m, (z * PLANE + q) * depth, depth)
        return pltpu.make_async_remote_copy(
            src_ref=ref, dst_ref=ref, send_sem=a2a_s.at[m, k], recv_sem=a2a_r.at[m, k],
            device_id=dev(q, z, c), device_id_type=MESH)

    def local(m):
        return pltpu.make_async_copy(piece_src(m, p), weight_dst(m, f * depth, depth), loc_sem.at[m])

    half = pl.ds(pl.multiple_of(c * rows, 16), rows)
    part_rows = (pl.ds(0, rows // 2), pl.ds(rows // 2, rows // 2))

    def tok_part(k, h):
        ref = psend.at[k, part_rows[h], :]
        if k == 0:
            source, to = psend.at[1 + h, part_rows[h], :], member(2 - h)
        else:
            start = pl.multiple_of(c * rows + h * (rows // 2), 16)
            source, to = tok_hbm.at[pl.ds(start, rows // 2), :], member(k)
        return pltpu.make_async_remote_copy(
            src_ref=source, dst_ref=ref, send_sem=tok_s.at[k, h], recv_sem=tok_r.at[k, h],
            device_id=dev(to, z, c), device_id_type=MESH)

    own_tok = pltpu.make_async_copy(tok_hbm.at[half, :], tok.at[3], loc_sem.at[3])

    def along(m, zs, step):
        ref = weight_dst(m, zs * unit, unit)
        sems = up_s if step > 0 else dn_s
        return pltpu.make_async_remote_copy(
            src_ref=ref, dst_ref=ref, send_sem=sems.at[m, zs], recv_sem=z_r.at[m, zs],
            device_id=dev(p, z + step, c), device_id_type=MESH)

    def to_sibling(m, zs):
        ref = weight_dst(m, zs * unit, unit)
        return pltpu.make_async_remote_copy(
            src_ref=ref, dst_ref=ref, send_sem=sib_s.at[m, zs], recv_sem=sib_r.at[m, zs],
            device_id=(f, 1 - c), device_id_type=MESH)

    def from_sibling(m, zs):
        ref = weight_sib(m, zs * unit, unit)
        return pltpu.make_async_remote_copy(
            src_ref=ref, dst_ref=ref, send_sem=sib_s.at[m, zs], recv_sem=sib_r.at[m, zs],
            device_id=(f, 1 - c), device_id_type=MESH)

    def forward(m, zs):
        @pl.when((zs <= z) & (z < nz - 1))
        def _():
            along(m, zs, 1).start()

        @pl.when((zs >= z) & (z > 0))
        def _():
            along(m, zs, -1).start()

        to_sibling(m, zs).start()

    def arrived(m, zs):
        along(m, zs, 1).wait_recv()

    def piece(m, k, step):
        ref = weight_dst(m, (z * PLANE + member(k)) * depth, depth)
        sems = up_s if step > 0 else dn_s
        return pltpu.make_async_remote_copy(
            src_ref=piece_src(m, p) if k == 3 else ref, dst_ref=ref,
            send_sem=sems.at[m, z], recv_sem=z_r.at[m, z],
            device_id=dev(p, z + step, c), device_id_type=MESH)

    def pass_piece(m, k):
        @pl.when(z < nz - 1)
        def _():
            piece(m, k, 1).start()

        @pl.when(z > 0)
        def _():
            piece(m, k, -1).start()

    for m in range(2):
        for k in (1, 2, 0):
            a2a(m, k).start()
        local(m).start()
        pass_piece(m, 3)
    for h in range(2):
        tok_part(1, h).start()
        tok_part(2, 1 - h).start()
    own_tok.start()

    def own_unit(m):
        if m == 2:
            pass_piece(m, 3)
        for k in (1, 2, 0):
            a2a_in(m, k).wait_recv()
            pass_piece(m, k)
        local(m).wait()
        to_sibling(m, z).start()

    own_unit(0)
    own_unit(1)

    side = z // (nz // 2)
    edge = z + side * (nz - 1 - 2 * z)
    late = (nz - 1) * (1 - side)
    inner = (z > 0) & (z < nz - 1)
    outer = jnp.logical_not(inner)

    def end_half(m, zs, h):
        ref = weight_dst(m, zs * unit + h * (unit // 2), unit // 2)
        return pltpu.make_async_remote_copy(
            src_ref=ref, dst_ref=ref, send_sem=end_s.at[m - 1, zs, h], recv_sem=end_r.at[m - 1, zs, h],
            device_id=dev(p, z + 2 * side - 1, c), device_id_type=MESH)

    def pair_half(m, zs, h, mine):
        where = weight_dst if mine else weight_sib
        ref = where(m, zs * unit + h * (unit // 2), unit // 2)
        return pltpu.make_async_remote_copy(
            src_ref=ref, dst_ref=ref, send_sem=pair_s.at[m - 1, zs, h], recv_sem=pair_r.at[m - 1, zs, h],
            device_id=(f, 1 - c), device_id_type=MESH)

    def across(zs, start, size):
        ref = weight_dst(2, start, size)
        return pltpu.make_async_remote_copy(
            src_ref=ref, dst_ref=ref, send_sem=mid_s.at[zs], recv_sem=z_r.at[2, zs],
            device_id=dev(p, z + 1 - 2 * side, c), device_id_type=MESH)

    def piece_out(q):
        start = (z * PLANE + q) * depth
        across(z, start, depth).start()
        ref = weight_dst(2, start, depth)
        half_at = 2 * q // PLANE
        pltpu.make_async_remote_copy(
            src_ref=ref, dst_ref=ref, send_sem=end_s.at[1, z, half_at], recv_sem=end_r.at[1, z, half_at],
            device_id=dev(p, z + 2 * side - 1, c), device_id_type=MESH).start()

    def own_down():
        for k in (1, 2, 0):
            a2a_in(2, k).wait_recv()
        local(2).wait()
        to_sibling(2, z).start()

        @pl.when(outer)
        def _():
            for k in range(PLANE):
                pass_piece(2, k)

        @pl.when(inner)
        def _():
            for q in range(PLANE):
                piece_out(q)

    def relay(m, d):
        @pl.when(z - d >= 0)
        def _():
            arrived(m, z - d)
            forward(m, z - d)

        @pl.when(z + d < nz)
        def _():
            arrived(m, z + d)
            forward(m, z + d)

    def relay_far(m):
        @pl.when(inner)
        def _():
            arrived(m, late)
            for h in range(2):
                end_half(m, late, h).start()
            to_sibling(m, late).start()

    def relay_near():
        @pl.when(inner)
        def _():
            zs = z + 1 - 2 * side
            arrived(2, zs)
            for h in range(2):
                end_half(2, zs, h).start()
            to_sibling(2, zs).start()
            zs = z + 2 * side - 1
            arrived(2, zs)
            across(zs, zs * unit, unit).start()
            to_sibling(2, zs).start()

    def take(m, d):
        @pl.when(outer)
        def _():
            zs = z + d * (1 - 2 * side)
            arrived(m, zs)
            to_sibling(m, zs).start()

    def take_half(m, zs, h):
        @pl.when(outer)
        def _():
            end_half(m, zs, h).wait_recv()
            pair_half(m, zs, h, True).start()

    def paired_half(m, zs, h):
        @pl.when(outer)
        def _():
            pair_half(m, zs, h, False).wait_recv()

        if h == 0:
            @pl.when(inner)
            def _():
                from_sibling(m, zs).wait_recv()

    def normalize(k):
        raw = tok.at[k] if k == 3 else psend.at[k]
        block = rows // 6

        @pl.loop(0, 6)
        def _(i):
            at = pl.ds(pl.multiple_of(i * block, 16), block)
            values = raw[at, :].astype(jnp.float32)
            scale = lax.rsqrt(jnp.mean(values * values, axis=-1, keepdims=True) + 1e-06)
            tok[k, at, :] = (values * scale * gain_ref[...]).astype(jnp.bfloat16)

    tiles = 2 * width // 256

    def tile_at(i):
        j = c * (tiles - 1) + i * (1 - 2 * c)
        return pl.ds(pl.multiple_of(j * 256, 256), 256)

    def project(m, k, at, start, size):
        depths = pl.ds(pl.multiple_of(start, 128), size)
        return jnp.dot(tok[k, :, depths], gu[m, depths, at], preferred_element_type=jnp.float32)

    def early(m, k):
        @pl.loop(0, tiles)
        def _(i):
            at = tile_at(i)
            acc[m, k, :, at] = project(m, k, at, side * unit, (nz - 1) * unit)

    def all_paired(m):
        for i in range(nz - 1):
            from_sibling(m, side + i).wait_recv()

    relay(0, 1)
    relay(1, 1)
    for h in range(2):
        tok_part(1 + h, h).wait_recv()
        tok_part(0, h).start()
    for k in (1, 2, 0):
        a2a(2, k).start()
    local(2).start()
    own_tok.wait()
    normalize(3)
    relay(0, nz - 2)

    def gated(k, start, size, add):
        @pl.loop(0, tiles)
        def _(i):
            at = tile_at(i)
            gate = project(0, k, at, start, size)
            if add:
                gate = acc[0, k, :, at] + gate
            acc[0, k, :, at] = gate / (1.0 + jnp.exp(-gate))

    def make_hidden(k, low, high):
        @pl.loop(low, high)
        def _(i):
            at = tile_at(i)
            up = acc[1, k, :, at] + project(1, k, at, late * unit + unit // 2, unit // 2)
            hidden[k, :, at] = (acc[0, k, :, at] * up).astype(jnp.bfloat16)

    def neighbours_tokens():
        for k in (1, 2):
            tok_part(k, 2 - k).wait_recv()
            normalize(k)

    def diagonal_tokens():
        for h in range(2):
            tok_part(0, h).wait_recv()
        normalize(0)

    @pl.when(inner)
    def _():
        all_paired(0)
        from_sibling(0, late).wait_recv()

        def whole_hidden(k):
            @pl.loop(0, tiles)
            def _(i):
                at = tile_at(i)
                up = project(1, k, at, 0, nz * unit)
                hidden[k, :, at] = (acc[0, k, :, at] * up).astype(jnp.bfloat16)

        gated(3, 0, nz * unit, False)
        neighbours_tokens()
        gated(1, 0, nz * unit, False)
        relay_far(1)
        gated(2, 0, nz * unit, False)
        all_paired(1)
        from_sibling(1, late).wait_recv()
        for k in (1, 2):
            whole_hidden(k)
        diagonal_tokens()
        gated(0, 0, nz * unit, False)
        own_down()
        whole_hidden(0)

    @pl.when(outer)
    def _():
        all_paired(0)
        early(0, 3)
        for k in (1, 2):
            tok_part(k, 2 - k).wait_recv()
            normalize(k)
            early(0, k)
        take(1, nz - 2)
        all_paired(1)
        for k in (3, 1, 2):
            early(1, k)
        diagonal_tokens()
        for m in range(2):
            early(m, 0)

        take(0, nz - 1)
        own_down()
        from_sibling(0, late).wait_recv()
        for k in range(PLANE):
            gated(k, late * unit, unit, True)
        take_half(1, late, 0)
        pair_half(1, late, 0, False).wait_recv()
        for k in range(PLANE):
            @pl.loop(0, tiles)
            def _(i):
                at = tile_at(i)
                acc[1, k, :, at] += project(1, k, at, late * unit, unit // 2)

        take_half(1, late, 1)
        for k in range(3):
            make_hidden(k, 0, tiles // 2)
        pair_half(1, late, 1, False).wait_recv()
        make_hidden(0, tiles // 2, tiles)

    for h in range(2):
        tok_part(0, h).wait_send()

    def first(h, step):
        at = (0, part_rows[h], columns_at(step))
        return pltpu.make_async_remote_copy(
            src_ref=psend.at[at], dst_ref=precv.at[at],
            send_sem=one_s.at[h, step], recv_sem=one_r.at[h, step],
            device_id=dev(member(1 + h), z, c), device_id_type=MESH)

    def last(k, h, step):
        at = (k, part_rows[h], columns_at(step))
        return pltpu.make_async_remote_copy(
            src_ref=psend.at[at], dst_ref=precv.at[at],
            send_sem=rs_s.at[2 * k + h - 2, step], recv_sem=rs_r.at[2 * k + h - 2, step],
            device_id=dev(member(k), z, c), device_id_type=MESH)

    def plane_at(step):
        near = (2 * edge - step + nz) // nz
        ahead = near * (1 - 2 * (step % 2)) * ((step + 1) // 2) + (1 - near) * (step - edge)
        return z + ahead * (1 - 2 * side)

    def columns_at(i):
        size = unit // 2
        return pl.ds(pl.multiple_of(plane_at(i // 2) * unit + i % 2 * size, 128), size)

    def add_and_send(step):
        for h in range(2):
            k = 2 - h
            first(h, step).wait_recv()
            at = (part_rows[h], columns_at(step))
            psend[(k, *at)] = (
                psend[(k, *at)].astype(jnp.float32) + precv[(0, *at)].astype(jnp.float32)
            ).astype(jnp.bfloat16)
            last(k, h, step).start()

    def partials(i):
        start = plane_at(i // 2) * unit + i % 2 * (unit // 2)

        def down(low, high):
            @pl.loop(0, unit // 512)
            def _(j):
                at = pl.ds(pl.multiple_of(start + j * 256, 256), 256)
                left = hidden[low:high].reshape((high - low) * rows, 2 * width)
                part = jnp.dot(left, dn[:, at], preferred_element_type=jnp.float32)
                for k in range(low, high):
                    block = part[(k - low) * rows:(k - low + 1) * rows]
                    if k == 3:
                        own[:, at] = block
                    else:
                        psend[k, :, at] = block.astype(jnp.bfloat16)

        down(0, 1)
        first(0, i).start()
        first(1, i).start()
        if i == 0:
            @pl.when(outer)
            def _():
                make_hidden(1, tiles // 2, tiles)
                make_hidden(2, tiles // 2, tiles)

            down(1, 3)
        else:
            down(1, 4)
        if i < 2:
            @pl.when(outer)
            def _():
                for k in (1, 2):
                    leave(k, i).start()

            @pl.when(inner)
            def _():
                last(1, 0, i).start()
                last(2, 1, i).start()
        else:
            last(1, 0, i).start()
            last(2, 1, i).start()
        if i == 0:
            @pl.when(outer)
            def _():
                make_hidden(3, 0, tiles)

            @pl.when(inner)
            def _():
                @pl.loop(0, tiles)
                def _(i):
                    at = tile_at(i)
                    up = project(1, 3, at, 0, nz * unit)
                    hidden[3, :, at] = (acc[0, 3, :, at] * up).astype(jnp.bfloat16)

            down(3, 4)

    def stage(number, k, i, to, src, dst, arrival):
        return pltpu.make_async_remote_copy(
            src_ref=src, dst_ref=dst, send_sem=det_s.at[number, k - 1, i], recv_sem=arrival,
            device_id=to, device_id_type=MESH)

    def leave(k, i):
        return stage(0, k, i, dev(p, z + 1 - 2 * side, c), psend.at[k, part_rows[k - 1], columns_at(i)],
                     detour.at[0, k - 1, i], det_r.at[0, k - 1, i])

    def cross(k, i):
        return stage(1, k, i, dev(member(k), z, c), detour.at[0, k - 1, i],
                     detour.at[1, k - 1, i], det_r.at[1, k - 1, i])

    def come_back(k, i):
        zs = z + 2 * side - 1
        start = pl.multiple_of(zs * unit + i * (unit // 2), 128)
        return stage(2, k, i, dev(p, zs, c), detour.at[1, k - 1, i],
                     precv.at[k, part_rows[k - 1], pl.ds(start, unit // 2)], rs_r.at[3 * k - 3, i])

    from_sibling(2, z).wait_recv()
    final = 2 * nz - 1
    for i in range(final + 1):
        if i > 1:
            paired_half(2, plane_at(i // 2), i % 2)
        partials(i)
        if i == 1:
            add_and_send(0)
            relay_near()

            @pl.when(inner)
            def _():
                add_and_send(1)
        elif i == 2:
            @pl.when(outer)
            def _():
                add_and_send(1)
        elif i > 2:
            add_and_send(i - 1)
        if i == 4:
            @pl.when(inner)
            def _():
                for j in range(2):
                    for k in (1, 2):
                        leave(k, j).wait_recv()
                        cross(k, j).start()
        if i == 5:
            relay_far(2)
        if i == 7:
            @pl.when(inner)
            def _():
                for j in range(2):
                    for k in (1, 2):
                        cross(k, j).wait_recv()
                        come_back(k, j).start()
        if 0 < i < final:
            take_half(2, plane_at((i + 1) // 2), (i + 1) % 2)
    add_and_send(final)

    for i in range(final + 1):
        at = columns_at(i)
        for k in (1, 2):
            for h in range(2):
                last(k, h, i).wait_recv()
        total = own[:, at]
        for k in (1, 2):
            total = total + precv[k, :, at].astype(jnp.float32)
        out_ref[:, at] = total.astype(out_ref.dtype)

    for m in range(3):
        for k in range(3):
            a2a(m, k).wait_send()
        for zs in range(nz):
            whole = (zs >= 0, (zs - late) * (zs - late) > 0, zs == z)[m]

            @pl.when(inner | whole)
            def _():
                to_sibling(m, zs).wait_send()

            @pl.when((zs <= z) & (z < nz - 1) & (outer | whole if m < 2 else outer))
            def _():
                along(m, zs, 1).wait_send()

            @pl.when((zs >= z) & (z > 0) & (outer | whole if m < 2 else outer))
            def _():
                along(m, zs, -1).wait_send()
    for h in range(2):
        @pl.when(inner)
        def _():
            end_half(1, late, h).wait_send()
            for zs in (z, z + 1 - 2 * side, late):
                end_half(2, zs, h).wait_send()

        @pl.when(outer)
        def _():
            pair_half(1, late, h, True).wait_send()
            for d in range(1, nz):
                pair_half(2, z + d * (1 - 2 * side), h, True).wait_send()

    @pl.when(inner)
    def _():
        for zs in (z, z + 2 * side - 1):
            across(zs, zs * unit, unit).wait_send()
    for k in (1, 2):
        for h in range(2):
            tok_part(k, h).wait_send()
    for i in range(final + 1):
        for h in range(2):
            first(h, i).wait_send()
            for k in (1, 2):
                if i < 2 and h == k - 1:
                    @pl.when(inner)
                    def _():
                        last(k, h, i).wait_send()
                        cross(k, i).wait_send()
                        come_back(k, i).wait_send()

                    @pl.when(outer)
                    def _():
                        leave(k, i).wait_send()
                else:
                    last(k, h, i).wait_send()


def fused(nfs, tokens, norm_gain, gate_weight, up_weight, down_weight):
    nz = nfs // PLANE
    features = tokens.shape[1]
    rows = tokens.shape[0] // 2
    width = gate_weight.shape[1] // PLANE
    any_spec = pl.BlockSpec(memory_space=pl.ANY)
    vmem_spec = pl.BlockSpec(memory_space=pltpu.VMEM)
    dma = pltpu.SemaphoreType.DMA
    bf16 = jnp.bfloat16
    return pl.pallas_call(
        functools.partial(kernel, nz),
        out_shape=pltpu.VMEM((rows, features), bf16),
        in_specs=[any_spec, vmem_spec, any_spec, any_spec, any_spec],
        out_specs=vmem_spec,
        scratch_shapes=[
            pltpu.VMEM((PLANE, rows, features), bf16),
            pltpu.VMEM((2, PLANE, rows, 2 * width), jnp.float32),
            pltpu.VMEM((2, features, 2 * width), bf16),
            pltpu.VMEM((2 * width, features), bf16),
            pltpu.VMEM((PLANE, rows, 2 * width), bf16),
            pltpu.VMEM((3, rows, features), bf16),
            pltpu.VMEM((3, rows, features), bf16),
            pltpu.VMEM((rows, features), jnp.float32),
            pltpu.VMEM((2, 2, 2, rows // 2, features // (2 * nz)), bf16),
            dma((4,)), dma((3, 3)), dma((3, 3)), dma((3, 2)), dma((3, 2)),
            dma((3, nz)), dma((3, nz)), dma((3, nz)), dma((3, nz)), dma((3, nz)),
            dma((2, nz, 2)), dma((2, nz, 2)), dma((2, nz, 2)), dma((2, nz, 2)), dma((nz,)),
            dma((2, 2 * nz)), dma((2, 2 * nz)), dma((4, 2 * nz)), dma((4, 2 * nz)),
            dma((3, 2, 2)), dma((2, 2, 2)),
        ],
        compiler_params=pltpu.CompilerParams(
            collective_id=0, has_side_effects=True, vmem_limit_bytes=60 * 1024 * 1024
        ),
    )(tokens, norm_gain.reshape(1, features), gate_weight, up_weight, down_weight)


def per_device(nfs, ntp, tokens, norm_gain, gate_weight, up_weight, down_weight):
    rows, depth = tokens.shape[0] // 2, gate_weight.shape[0]
    fits = (
        ntp == 2
        and nfs % PLANE == 0
        and nfs == PLANE * PLANE
        and rows % 96 == 0
        and depth % 128 == 0
        and depth * nfs == tokens.shape[1]
        and gate_weight.shape[1] % (PLANE * 128) == 0
    )
    body = functools.partial(fused, nfs) if fits else simple
    return body(tokens, norm_gain, gate_weight, up_weight, down_weight)


def solution(mesh):
    in_specs = (P("fs", None), P(), P("fs", "tp"), P("fs", "tp"), P("tp", "fs"))
    out_specs = P(("fs", "tp"), None)
    body = functools.partial(per_device, mesh.shape["fs"], mesh.shape["tp"])
    return jax.shard_map(
        body, mesh=mesh, in_specs=in_specs, out_specs=out_specs, check_vma=False
    )
```

```python
import functools

import jax
import jax.numpy as jnp
from jax import lax
from jax.experimental import pallas as pl
from jax.experimental.pallas import tpu as pltpu
from jax.sharding import PartitionSpec as P

MESH = pl.DeviceIdType.MESH
PLANE = 4
ORDER = ((1, 1), (0, 1), (1, 0), (0, 0))


def simple(tokens, norm_gain, gate_weight, up_weight, down_weight):
    values = tokens.astype(jnp.float32)
    scale = lax.rsqrt(jnp.mean(values * values, axis=-1, keepdims=True) + 1e-06)
    normed = (values * scale * norm_gain).astype(jnp.bfloat16)

    def project(piece):
        whole = lax.all_gather(piece, "fs", axis=0, tiled=True)
        return jnp.dot(normed, whole, preferred_element_type=jnp.float32)

    hidden = (jax.nn.silu(project(gate_weight)) * project(up_weight)).astype(jnp.bfloat16)
    down_whole = lax.all_gather(down_weight, "fs", axis=1, tiled=True)
    return lax.psum_scatter(
        jnp.dot(hidden, down_whole, preferred_element_type=jnp.float32).astype(jnp.bfloat16),
        "tp",
        scatter_dimension=0,
        tiled=True,
    )


def kernel(nz, tok_hbm, gain_hbm, gate_hbm, up_hbm, down_hbm, out_ref,
           gain_ref, tok, acc, gu, dn, hidden, psend, precv, own, detour,
           loc_sem, a2a_s, a2a_r, tok_s, tok_r, up_s, dn_s, z_r, sib_s, sib_r, end_s, end_r, pair_s, pair_r, mid_s,
           one_s, one_r, rs_s, rs_r, det_s, det_r):
    f = lax.axis_index("fs")
    c = lax.axis_index("tp")
    z, p = f // PLANE, f % PLANE
    y, x = p // 2, p % 2
    depth = gate_hbm.shape[0]
    width = gate_hbm.shape[1] // PLANE
    rows = tok_hbm.shape[0] // 2
    unit = depth * PLANE

    def member(k):
        oy, ox = ORDER[k]
        return ((y + oy) % 2) * 2 + (x + ox) % 2

    def dev(plane, z_, core):
        return (z_ * PLANE + plane, core)

    barrier = pltpu.get_barrier_semaphore()
    for k in range(3):
        pl.semaphore_signal(barrier, inc=1, device_id=dev(member(k), z, c), device_id_type=MESH)
    pl.semaphore_signal(barrier, inc=1, device_id=(f, 1 - c), device_id_type=MESH)

    @pl.when(z > 0)
    def _():
        pl.semaphore_signal(barrier, inc=1, device_id=dev(p, z - 1, c), device_id_type=MESH)

    @pl.when(z < nz - 1)
    def _():
        pl.semaphore_signal(barrier, inc=1, device_id=dev(p, z + 1, c), device_id_type=MESH)

    pl.semaphore_wait(barrier, 4 + (z + nz - 1) // nz + (2 * nz - 2 - z) // nz)

    sources = (gate_hbm, up_hbm, down_hbm)

    def piece_src(m, q):
        start = pl.multiple_of(q * width, 128)
        if m < 2:
            return sources[m].at[:, pl.ds(start, width)]
        return sources[m].at[pl.ds(start, width), :]

    def weight_dst(m, start, size):
        start = pl.multiple_of(start, 128)
        units = pl.ds(pl.multiple_of(c * width, 128), width)
        if m < 2:
            return gu.at[m, pl.ds(start, size), units]
        return dn.at[units, pl.ds(start, size)]

    def weight_sib(m, start, size):
        start = pl.multiple_of(start, 128)
        units = pl.ds(pl.multiple_of((1 - c) * width, 128), width)
        if m < 2:
            return gu.at[m, pl.ds(start, size), units]
        return dn.at[units, pl.ds(start, size)]

    def a2a(m, k):
        q = member(k)
        return pltpu.make_async_remote_copy(
            src_ref=piece_src(m, q), dst_ref=weight_dst(m, f * depth, depth),
            send_sem=a2a_s.at[m, k], recv_sem=a2a_r.at[m, k],
            device_id=dev(q, z, c), device_id_type=MESH)

    def a2a_in(m, k):
        q = member(k)
        ref = weight_dst(m, (z * PLANE + q) * depth, depth)
        return pltpu.make_async_remote_copy(
            src_ref=ref, dst_ref=ref, send_sem=a2a_s.at[m, k], recv_sem=a2a_r.at[m, k],
            device_id=dev(q, z, c), device_id_type=MESH)

    def local(m):
        return pltpu.make_async_copy(piece_src(m, p), weight_dst(m, f * depth, depth), loc_sem.at[m])

    half = pl.ds(pl.multiple_of(c * rows, 16), rows)
    part_rows = (pl.ds(0, rows // 2), pl.ds(rows // 2, rows // 2))

    def tok_part(k, h):
        ref = psend.at[k, part_rows[h], :]
        if k == 0:
            source, to = psend.at[1 + h, part_rows[h], :], member(2 - h)
        else:
            start = pl.multiple_of(c * rows + h * (rows // 2), 16)
            source, to = tok_hbm.at[pl.ds(start, rows // 2), :], member(k)
        return pltpu.make_async_remote_copy(
            src_ref=source, dst_ref=ref, send_sem=tok_s.at[k, h], recv_sem=tok_r.at[k, h],
            device_id=dev(to, z, c), device_id_type=MESH)

    own_tok = pltpu.make_async_copy(tok_hbm.at[half, :], tok.at[3], loc_sem.at[3])

    def along(m, zs, step):
        ref = weight_dst(m, zs * unit, unit)
        sems = up_s if step > 0 else dn_s
        return pltpu.make_async_remote_copy(
            src_ref=ref, dst_ref=ref, send_sem=sems.at[m, zs], recv_sem=z_r.at[m, zs],
            device_id=dev(p, z + step, c), device_id_type=MESH)

    def to_sibling(m, zs):
        ref = weight_dst(m, zs * unit, unit)
        return pltpu.make_async_remote_copy(
            src_ref=ref, dst_ref=ref, send_sem=sib_s.at[m, zs], recv_sem=sib_r.at[m, zs],
            device_id=(f, 1 - c), device_id_type=MESH)

    def from_sibling(m, zs):
        ref = weight_sib(m, zs * unit, unit)
        return pltpu.make_async_remote_copy(
            src_ref=ref, dst_ref=ref, send_sem=sib_s.at[m, zs], recv_sem=sib_r.at[m, zs],
            device_id=(f, 1 - c), device_id_type=MESH)

    def forward(m, zs):
        @pl.when((zs <= z) & (z < nz - 1))
        def _():
            along(m, zs, 1).start()

        @pl.when((zs >= z) & (z > 0))
        def _():
            along(m, zs, -1).start()

        to_sibling(m, zs).start()

    def arrived(m, zs):
        along(m, zs, 1).wait_recv()

    def piece(m, k, step):
        ref = weight_dst(m, (z * PLANE + member(k)) * depth, depth)
        sems = up_s if step > 0 else dn_s
        return pltpu.make_async_remote_copy(
            src_ref=piece_src(m, p) if k == 3 else ref, dst_ref=ref,
            send_sem=sems.at[m, z], recv_sem=z_r.at[m, z],
            device_id=dev(p, z + step, c), device_id_type=MESH)

    def pass_piece(m, k):
        @pl.when(z < nz - 1)
        def _():
            piece(m, k, 1).start()

        @pl.when(z > 0)
        def _():
            piece(m, k, -1).start()

    for m in range(2):
        for k in (1, 2, 0):
            a2a(m, k).start()
        local(m).start()
        pass_piece(m, 3)
    for h in range(2):
        tok_part(1, h).start()
        tok_part(2, 1 - h).start()
    own_tok.start()
    gain = pltpu.make_async_copy(gain_hbm, gain_ref, loc_sem.at[4])
    gain.start()

    def own_unit(m):
        if m == 2:
            pass_piece(m, 3)
        for k in (1, 2, 0):
            a2a_in(m, k).wait_recv()
            pass_piece(m, k)
        local(m).wait()
        to_sibling(m, z).start()

    own_unit(0)
    own_unit(1)

    side = z // (nz // 2)
    edge = z + side * (nz - 1 - 2 * z)
    late = (nz - 1) * (1 - side)
    inner = (z > 0) & (z < nz - 1)
    outer = jnp.logical_not(inner)

    def split(h, parts):
        if parts == 2 or h == 0:
            return h * (unit // 2), unit // 2
        return (h + 1) * (unit // 4), unit // 4

    def end_part(m, zs, h, parts):
        start, size = split(h, parts)
        ref = weight_dst(m, zs * unit + start, size)
        return pltpu.make_async_remote_copy(
            src_ref=ref, dst_ref=ref, send_sem=end_s.at[m - 1, zs, h], recv_sem=end_r.at[m - 1, zs, h],
            device_id=dev(p, z + 2 * side - 1, c), device_id_type=MESH)

    def pair_part(m, zs, h, parts, mine):
        where = weight_dst if mine else weight_sib
        start, size = split(h, parts)
        ref = where(m, zs * unit + start, size)
        return pltpu.make_async_remote_copy(
            src_ref=ref, dst_ref=ref, send_sem=pair_s.at[m - 1, zs, h], recv_sem=pair_r.at[m - 1, zs, h],
            device_id=(f, 1 - c), device_id_type=MESH)

    def across(zs, start, size):
        ref = weight_dst(2, start, size)
        return pltpu.make_async_remote_copy(
            src_ref=ref, dst_ref=ref, send_sem=mid_s.at[zs], recv_sem=z_r.at[2, zs],
            device_id=dev(p, z + 1 - 2 * side, c), device_id_type=MESH)

    def piece_out(q):
        start = (z * PLANE + q) * depth
        across(z, start, depth).start()
        ref = weight_dst(2, start, depth)
        half_at = 2 * q // PLANE
        pltpu.make_async_remote_copy(
            src_ref=ref, dst_ref=ref, send_sem=end_s.at[1, z, half_at], recv_sem=end_r.at[1, z, half_at],
            device_id=dev(p, z + 2 * side - 1, c), device_id_type=MESH).start()

    def own_down():
        for k in (1, 2, 0):
            a2a_in(2, k).wait_recv()
        local(2).wait()
        to_sibling(2, z).start()

        @pl.when(outer)
        def _():
            for k in range(PLANE):
                pass_piece(2, k)

        @pl.when(inner)
        def _():
            for q in range(PLANE):
                piece_out(q)

    def relay(m, d):
        @pl.when(z - d >= 0)
        def _():
            arrived(m, z - d)
            forward(m, z - d)

        @pl.when(z + d < nz)
        def _():
            arrived(m, z + d)
            forward(m, z + d)

    def relay_far(m):
        @pl.when(inner)
        def _():
            arrived(m, late)
            for h in range(m + 1):
                end_part(m, late, h, m + 1).start()
            to_sibling(m, late).start()

    def relay_near():
        @pl.when(inner)
        def _():
            zs = z + 1 - 2 * side
            arrived(2, zs)
            for h in range(2):
                end_part(2, zs, h, 2).start()
            to_sibling(2, zs).start()
            zs = z + 2 * side - 1
            arrived(2, zs)
            across(zs, zs * unit, unit).start()
            to_sibling(2, zs).start()

    def take(m, d):
        @pl.when(outer)
        def _():
            zs = z + d * (1 - 2 * side)
            arrived(m, zs)
            to_sibling(m, zs).start()

    def take_part(m, zs, h, parts):
        @pl.when(outer)
        def _():
            end_part(m, zs, h, parts).wait_recv()
            pair_part(m, zs, h, parts, True).start()

    def paired_part(m, zs, h, parts):
        @pl.when(outer)
        def _():
            pair_part(m, zs, h, parts, False).wait_recv()

        if h == 0:
            @pl.when(inner)
            def _():
                from_sibling(m, zs).wait_recv()

    def normalize(k):
        raw = tok.at[k] if k == 3 else psend.at[k]
        block = rows // 6

        @pl.loop(0, 6)
        def _(i):
            at = pl.ds(pl.multiple_of(i * block, 16), block)
            values = raw[at, :].astype(jnp.float32)
            scale = lax.rsqrt(jnp.mean(values * values, axis=-1, keepdims=True) + 1e-06)
            tok[k, at, :] = (values * scale * gain_ref[...]).astype(jnp.bfloat16)

    tiles = 2 * width // 256

    def tile_at(i):
        j = c * (tiles - 1) + i * (1 - 2 * c)
        return pl.ds(pl.multiple_of(j * 256, 256), 256)

    def project(m, k, at, start, size):
        depths = pl.ds(pl.multiple_of(start, 128), size)
        return jnp.dot(tok[k, :, depths], gu[m, depths, at], preferred_element_type=jnp.float32)

    def early(m, k):
        @pl.loop(0, tiles)
        def _(i):
            at = tile_at(i)
            acc[m, k, :, at] = project(m, k, at, side * unit, (nz - 1) * unit)

    def all_paired(m):
        for i in range(nz - 1):
            from_sibling(m, side + i).wait_recv()

    relay(0, 1)
    relay(1, 1)
    for h in range(2):
        tok_part(1 + h, h).wait_recv()
        tok_part(0, h).start()
    for k in (1, 2, 0):
        a2a(2, k).start()
    local(2).start()
    own_tok.wait()
    gain.wait()
    normalize(3)
    relay(0, nz - 2)

    def gated(k, start, size, add):
        @pl.loop(0, tiles)
        def _(i):
            at = tile_at(i)
            gate = project(0, k, at, start, size)
            if add:
                gate = acc[0, k, :, at] + gate
            acc[0, k, :, at] = gate / (1.0 + jnp.exp(-gate))

    def make_hidden(k, low, high):
        @pl.loop(low, high)
        def _(i):
            at = tile_at(i)
            up = acc[1, k, :, at] + project(1, k, at, late * unit + unit // 2, unit // 2)
            hidden[k, :, at] = (acc[0, k, :, at] * up).astype(jnp.bfloat16)

    def neighbours_tokens():
        for k in (1, 2):
            tok_part(k, 2 - k).wait_recv()
            normalize(k)

    def diagonal_tokens():
        for h in range(2):
            tok_part(0, h).wait_recv()
        normalize(0)

    @pl.when(inner)
    def _():
        all_paired(0)
        from_sibling(0, late).wait_recv()

        def whole_hidden(k):
            @pl.loop(0, tiles)
            def _(i):
                at = tile_at(i)
                up = project(1, k, at, 0, nz * unit)
                hidden[k, :, at] = (acc[0, k, :, at] * up).astype(jnp.bfloat16)

        gated(3, 0, nz * unit, False)
        neighbours_tokens()
        gated(1, 0, nz * unit, False)
        relay_far(1)
        gated(2, 0, nz * unit, False)
        all_paired(1)
        from_sibling(1, late).wait_recv()
        for k in (1, 2):
            whole_hidden(k)
        diagonal_tokens()
        gated(0, 0, nz * unit, False)
        own_down()
        whole_hidden(0)

    @pl.when(outer)
    def _():
        all_paired(0)
        early(0, 3)
        for k in (1, 2):
            tok_part(k, 2 - k).wait_recv()
            normalize(k)
            early(0, k)
        take(1, nz - 2)
        all_paired(1)
        for k in (3, 1, 2):
            early(1, k)
        diagonal_tokens()
        for m in range(2):
            early(m, 0)

        take(0, nz - 1)
        own_down()
        from_sibling(0, late).wait_recv()
        for k in range(PLANE):
            gated(k, late * unit, unit, True)
        take_part(1, late, 0, 2)
        pair_part(1, late, 0, 2, False).wait_recv()
        for k in range(PLANE):
            @pl.loop(0, tiles)
            def _(i):
                at = tile_at(i)
                acc[1, k, :, at] += project(1, k, at, late * unit, unit // 2)

        take_part(1, late, 1, 2)
        for k in range(3):
            make_hidden(k, 0, tiles // 2)
        pair_part(1, late, 1, 2, False).wait_recv()
        make_hidden(0, tiles // 2, tiles)

    for h in range(2):
        tok_part(0, h).wait_send()

    def first(h, step):
        at = (0, part_rows[h], columns_at(step))
        return pltpu.make_async_remote_copy(
            src_ref=psend.at[at], dst_ref=precv.at[at],
            send_sem=one_s.at[h, step], recv_sem=one_r.at[h, step],
            device_id=dev(member(1 + h), z, c), device_id_type=MESH)

    def last(k, h, step):
        at = (k, part_rows[h], columns_at(step))
        return pltpu.make_async_remote_copy(
            src_ref=psend.at[at], dst_ref=precv.at[at],
            send_sem=rs_s.at[2 * k + h - 2, step], recv_sem=rs_r.at[2 * k + h - 2, step],
            device_id=dev(member(k), z, c), device_id_type=MESH)

    def plane_at(step):
        near = (2 * edge - step + nz) // nz
        ahead = near * (1 - 2 * (step % 2)) * ((step + 1) // 2) + (1 - near) * (step - edge)
        return z + ahead * (1 - 2 * side)

    final = 2 * nz
    cuts = [(step, h, 2) for step in range(nz - 1) for h in range(2)] + [(nz - 1, h, 3) for h in range(3)]

    def columns_at(i):
        step, h, parts = cuts[i]
        start, size = split(h, parts)
        return pl.ds(pl.multiple_of(plane_at(step) * unit + start, 128), size)

    def add_and_send(step):
        for h in range(2):
            k = 2 - h
            first(h, step).wait_recv()
            at = (part_rows[h], columns_at(step))
            psend[(k, *at)] = (
                psend[(k, *at)].astype(jnp.float32) + precv[(0, *at)].astype(jnp.float32)
            ).astype(jnp.bfloat16)
            last(k, h, step).start()

    def partials(i):
        step, h, parts = cuts[i]
        start, size = split(h, parts)
        start, tile = plane_at(step) * unit + start, 128 if size % 256 else 256

        def down(low, high):
            @pl.loop(0, size // tile)
            def _(j):
                at = pl.ds(pl.multiple_of(start + j * tile, 128), tile)
                left = hidden[low:high].reshape((high - low) * rows, 2 * width)
                part = jnp.dot(left, dn[:, at], preferred_element_type=jnp.float32)
                for k in range(low, high):
                    block = part[(k - low) * rows:(k - low + 1) * rows]
                    if k == 3:
                        own[:, at] = block
                    else:
                        psend[k, :, at] = block.astype(jnp.bfloat16)

        down(0, 1)
        first(0, i).start()
        first(1, i).start()
        if i == final:
            last(1, 0, i - 1).start()
            last(2, 1, i - 1).start()
        if i == 0:
            @pl.when(outer)
            def _():
                make_hidden(1, tiles // 2, tiles)
                make_hidden(2, tiles // 2, tiles)

            down(1, 3)
        else:
            down(1, 4)
        if i < 2:
            @pl.when(outer)
            def _():
                for k in (1, 2):
                    leave(k, i).start()

            @pl.when(inner)
            def _():
                last(1, 0, i).start()
                last(2, 1, i).start()
        elif i != final - 1:
            last(1, 0, i).start()
            last(2, 1, i).start()
        if i == 0:
            @pl.when(outer)
            def _():
                make_hidden(3, 0, tiles)

            @pl.when(inner)
            def _():
                @pl.loop(0, tiles)
                def _(i):
                    at = tile_at(i)
                    up = project(1, 3, at, 0, nz * unit)
                    hidden[3, :, at] = (acc[0, 3, :, at] * up).astype(jnp.bfloat16)

            down(3, 4)

    def stage(number, k, i, to, src, dst, arrival):
        return pltpu.make_async_remote_copy(
            src_ref=src, dst_ref=dst, send_sem=det_s.at[number, k - 1, i], recv_sem=arrival,
            device_id=to, device_id_type=MESH)

    def leave(k, i):
        return stage(0, k, i, dev(p, z + 1 - 2 * side, c), psend.at[k, part_rows[k - 1], columns_at(i)],
                     detour.at[0, k - 1, i], det_r.at[0, k - 1, i])

    def cross(k, i):
        return stage(1, k, i, dev(member(k), z, c), detour.at[0, k - 1, i],
                     detour.at[1, k - 1, i], det_r.at[1, k - 1, i])

    def come_back(k, i):
        zs = z + 2 * side - 1
        start = pl.multiple_of(zs * unit + i * (unit // 2), 128)
        return stage(2, k, i, dev(p, zs, c), detour.at[1, k - 1, i],
                     precv.at[k, part_rows[k - 1], pl.ds(start, unit // 2)], rs_r.at[3 * k - 3, i])

    from_sibling(2, z).wait_recv()
    for i in range(final + 1):
        if i > 1:
            paired_part(2, plane_at(cuts[i][0]), *cuts[i][1:])
        partials(i)
        if i == 1:
            add_and_send(0)
            relay_near()

            @pl.when(inner)
            def _():
                add_and_send(1)
        elif i == 2:
            @pl.when(outer)
            def _():
                add_and_send(1)
        elif i > 2:
            add_and_send(i - 1)
        if i == 4:
            @pl.when(inner)
            def _():
                for j in range(2):
                    for k in (1, 2):
                        leave(k, j).wait_recv()
                        cross(k, j).start()
        if i == 5:
            relay_far(2)
        if i == 7:
            @pl.when(inner)
            def _():
                for j in range(2):
                    for k in (1, 2):
                        cross(k, j).wait_recv()
                        come_back(k, j).start()
        if 0 < i < final:
            take_part(2, plane_at(cuts[i + 1][0]), *cuts[i + 1][1:])
    add_and_send(final)

    for i in range(final + 1):
        at = columns_at(i)
        for k in (1, 2):
            for h in range(2):
                last(k, h, i).wait_recv()
        total = own[:, at]
        for k in (1, 2):
            total = total + precv[k, :, at].astype(jnp.float32)
        out_ref[:, at] = total.astype(out_ref.dtype)

    for m in range(3):
        for k in range(3):
            a2a(m, k).wait_send()
        for zs in range(nz):
            whole = (zs >= 0, (zs - late) * (zs - late) > 0, zs == z)[m]

            @pl.when(inner | whole)
            def _():
                to_sibling(m, zs).wait_send()

            @pl.when((zs <= z) & (z < nz - 1) & (outer | whole if m < 2 else outer))
            def _():
                along(m, zs, 1).wait_send()

            @pl.when((zs >= z) & (z > 0) & (outer | whole if m < 2 else outer))
            def _():
                along(m, zs, -1).wait_send()
    pieces = [(1, nz - 1, h, 2) for h in range(2)] + [(2, nz - 1, h, 3) for h in range(3)]
    pieces += [(2, d, h, 2) for d in range(1, nz - 1) for h in range(2)]
    for m, d, h, parts in pieces:
        @pl.when(inner)
        def _():
            zs = late if d == nz - 1 else z + (d - 1) * (1 - 2 * side)
            end_part(m, zs, h, parts).wait_send()

        @pl.when(outer)
        def _():
            pair_part(m, z + d * (1 - 2 * side), h, parts, True).wait_send()

    @pl.when(inner)
    def _():
        for zs in (z, z + 2 * side - 1):
            across(zs, zs * unit, unit).wait_send()
    for k in (1, 2):
        for h in range(2):
            tok_part(k, h).wait_send()
    for i in range(final + 1):
        for h in range(2):
            first(h, i).wait_send()
            for k in (1, 2):
                if i < 2 and h == k - 1:
                    @pl.when(inner)
                    def _():
                        last(k, h, i).wait_send()
                        cross(k, i).wait_send()
                        come_back(k, i).wait_send()

                    @pl.when(outer)
                    def _():
                        leave(k, i).wait_send()
                else:
                    last(k, h, i).wait_send()


def fused(nfs, tokens, norm_gain, gate_weight, up_weight, down_weight):
    nz = nfs // PLANE
    features = tokens.shape[1]
    rows = tokens.shape[0] // 2
    width = gate_weight.shape[1] // PLANE
    any_spec = pl.BlockSpec(memory_space=pl.ANY)
    vmem_spec = pl.BlockSpec(memory_space=pltpu.VMEM)
    dma = pltpu.SemaphoreType.DMA
    bf16 = jnp.bfloat16
    return pl.pallas_call(
        functools.partial(kernel, nz),
        out_shape=pltpu.VMEM((rows, features), bf16),
        in_specs=[any_spec] * 5,
        out_specs=vmem_spec,
        scratch_shapes=[
            pltpu.VMEM((1, features), jnp.float32),
            pltpu.VMEM((PLANE, rows, features), bf16),
            pltpu.VMEM((2, PLANE, rows, 2 * width), jnp.float32),
            pltpu.VMEM((2, features, 2 * width), bf16),
            pltpu.VMEM((2 * width, features), bf16),
            pltpu.VMEM((PLANE, rows, 2 * width), bf16),
            pltpu.VMEM((3, rows, features), bf16),
            pltpu.VMEM((3, rows, features), bf16),
            pltpu.VMEM((rows, features), jnp.float32),
            pltpu.VMEM((2, 2, 2, rows // 2, features // (2 * nz)), bf16),
            dma((5,)), dma((3, 3)), dma((3, 3)), dma((3, 2)), dma((3, 2)),
            dma((3, nz)), dma((3, nz)), dma((3, nz)), dma((3, nz)), dma((3, nz)),
            dma((2, nz, 3)), dma((2, nz, 3)), dma((2, nz, 3)), dma((2, nz, 3)), dma((nz,)),
            dma((2, 2 * nz + 1)), dma((2, 2 * nz + 1)), dma((4, 2 * nz + 1)), dma((4, 2 * nz + 1)),
            dma((3, 2, 2)), dma((2, 2, 2)),
        ],
        compiler_params=pltpu.CompilerParams(
            collective_id=0, has_side_effects=True, vmem_limit_bytes=60 * 1024 * 1024
        ),
    )(tokens, norm_gain.reshape(1, features), gate_weight, up_weight, down_weight)


def per_device(nfs, ntp, tokens, norm_gain, gate_weight, up_weight, down_weight):
    rows, depth = tokens.shape[0] // 2, gate_weight.shape[0]
    fits = (
        ntp == 2
        and nfs % PLANE == 0
        and nfs == PLANE * PLANE
        and rows % 96 == 0
        and depth % 128 == 0
        and depth * nfs == tokens.shape[1]
        and gate_weight.shape[1] % (PLANE * 128) == 0
    )
    body = functools.partial(fused, nfs) if fits else simple
    return body(tokens, norm_gain, gate_weight, up_weight, down_weight)


def solution(mesh):
    in_specs = (P("fs", None), P(), P("fs", "tp"), P("fs", "tp"), P("tp", "fs"))
    out_specs = P(("fs", "tp"), None)
    body = functools.partial(per_device, mesh.shape["fs"], mesh.shape["tp"])
    return jax.shard_map(
        body, mesh=mesh, in_specs=in_specs, out_specs=out_specs, check_vma=False
    )
```
